256 devices in a mesh: sp: 64 (over z, x, core), tp: 4 (over y).
Axes of the slice: x: 4, y: 4, z: 8, core: 2. Of those that a mesh axis runs over, the one named last changes fastest.
Arguments:
- inputs: bfloat16 [32768, 2048], P('sp', 'tp'), may hold values from -45 to 45
- norm_gain: float32 [3, 2048], replicated, may hold values from 0.1 to 1.9
- w_value: bfloat16 [3, 2048, 1024], P(None, 'sp', 'tp'), may hold values from -0.125 to 0.125
- w_gate: bfloat16 [3, 2048, 1024], P(None, 'sp', 'tp'), may hold values from -0.125 to 0.125
- conv_taps: float32 [3, 31, 1024], P(None, None, 'tp'), may hold values from -5 to 5
- ln_gain: float32 [3, 1024], P(None, 'tp'), may hold values from 0.1 to 1.9
- ln_bias: float32 [3, 1024], P(None, 'tp'), may hold values from -3 to 3
- w_out: bfloat16 [3, 1024, 2048], P(None, 'tp', 'sp'), may hold values from -0.1875 to 0.1875
Outputs:
- stream: bfloat16 [32768, 2048], P('sp', 'tp')
The draws below stay inside these ranges and needn't reach their ends.
All inputs are finite; a program needn't handle non-finite values.
Results may differ from the reference program's by a relative error of at most 0.01.
Values may be sent and summed in bfloat16 or wider, within the bound.
No kernel may reach another device: no remote copies, remote signals or barrier semaphores. Data moves between devices by JAX's collectives and lax.ppermute only.
A program may use at most 64 MiB of HBM per device.

```python
import jax
import jax.numpy as jnp
from jax import lax

D = 2048
C = 1024
K = 31
LAYERS = 3
TOKENS = 32768
N_TP = 4


def draw_inputs(key, part):
    key_a, key_b = jax.random.split(jax.random.fold_in(key, 11), 2)
    ramp = 10.0 ** (0.5 * jnp.arange(D, dtype=jnp.float32) / D + 0.3 * jax.random.uniform(key_b, (D,), jnp.float32))
    base = jnp.clip(jax.random.normal(key_a, (TOKENS, D), jnp.float32), -4.0, 4.0)
    return (base * ramp[None, :]).astype(jnp.bfloat16)


def draw_conv_taps(key, part):
    key_a, key_b = jax.random.split(jax.random.fold_in(key, 23), 2)
    ramp = K ** (-0.5) * 10.0 ** (0.5 * jnp.arange(C, dtype=jnp.float32) / C + 0.3 * jax.random.uniform(key_b, (LAYERS, 1, C), jnp.float32))
    base = jnp.clip(jax.random.normal(key_a, (LAYERS, K, C), jnp.float32), -4.0, 4.0)
    return base * ramp


def levels(key, shape, cuts, low, high):
    factor_of = 1.0
    for dim, blocks in cuts:
        draws = jax.random.uniform(jax.random.fold_in(jax.random.fold_in(key, 6), dim), (blocks,), jnp.float32, low / len(cuts), high / len(cuts))
        factor_of = factor_of * jnp.repeat(jnp.exp(draws), shape[dim] // blocks).reshape((-1,) + (1,) * (len(shape) - 1 - dim))
    return factor_of


def normal_values(stream_key, shape, width, bound, cuts=(), kind=jnp.bfloat16):
    loudness = levels(stream_key, shape, cuts, -0.22, 0.18) if cuts else 1.0
    values = jax.random.normal(stream_key, shape, jnp.float32) * width * loudness
    return jnp.minimum(jnp.maximum(values, -bound), bound).astype(kind)


def setup_inputs(seed: int = 0) -> dict:
    streams_of = jax.random.split(jax.random.key(seed), 9)
    inputs = draw_inputs(jax.random.fold_in(streams_of[8], 71), 0)
    norm_gain = jnp.clip(1.0 + 0.18 * jax.random.normal(streams_of[1], (LAYERS, D), jnp.float32), 0.1, 1.9)
    w_value = normal_values(streams_of[2], (LAYERS, D, C), D ** -0.5, 0.125, ((1, 64), (2, 4)))
    w_gate = normal_values(streams_of[3], (LAYERS, D, C), D ** -0.5, 0.125, ((1, 64), (2, 4)))
    conv_taps = draw_conv_taps(jax.random.fold_in(streams_of[8], 71), 0)
    ln_gain = jnp.clip(1.0 + 0.18 * jax.random.normal(streams_of[5], (LAYERS, C), jnp.float32), 0.1, 1.9)
    ln_bias = normal_values(streams_of[6], (LAYERS, C), 0.5, 3.0, ((1, 4),), jnp.float32)
    w_out = normal_values(streams_of[7], (LAYERS, C, D), C ** -0.5, 0.1875, ((1, 4), (2, 64)))
    return {"inputs": inputs, "norm_gain": norm_gain, "w_value": w_value, "w_gate": w_gate, "conv_taps": conv_taps, "ln_gain": ln_gain, "ln_bias": ln_bias, "w_out": w_out}


def reference(inputs, norm_gain, w_value, w_gate, conv_taps, ln_gain, ln_bias, w_out):
    block = C // N_TP
    stream = inputs
    for layer in range(LAYERS):
        xf = stream.astype(jnp.float32)
        meansq = lax.optimization_barrier(jnp.mean(xf * xf, axis=1, keepdims=True))
        hidden = (xf * lax.rsqrt(meansq + 1e-06) * norm_gain[layer][None, :]).astype(jnp.bfloat16)
        value = jnp.dot(hidden, w_value[layer], preferred_element_type=jnp.float32)
        gate = jnp.dot(hidden, w_gate[layer], preferred_element_type=jnp.float32)
        glu = (value * jax.nn.sigmoid(gate)).astype(jnp.bfloat16)
        padded = jnp.pad(glu.astype(jnp.float32), ((K - 1, 0), (0, 0)))
        filtered = jnp.zeros((TOKENS, C), jnp.float32)
        for tap in range(K):
            filtered = filtered + conv_taps[layer, tap][None, :] * padded[tap:tap + TOKENS]
        mean_val = lax.optimization_barrier(jnp.mean(filtered, axis=1, keepdims=True))
        var_val = lax.optimization_barrier(jnp.mean(filtered * filtered, axis=1, keepdims=True)) - mean_val * mean_val
        normed = jax.nn.silu((filtered - mean_val) * lax.rsqrt(var_val + 1e-06) * ln_gain[layer][None, :] + ln_bias[layer][None, :]).astype(jnp.bfloat16)
        branch = jnp.zeros((TOKENS, D), jnp.float32)
        for part_index in range(N_TP):
            piece = jnp.dot(normed[:, part_index * block:(part_index + 1) * block], w_out[layer, part_index * block:(part_index + 1) * block], preferred_element_type=jnp.float32).astype(jnp.bfloat16)
            branch = branch + piece.astype(jnp.float32)
        stream = (xf + branch).astype(jnp.bfloat16)
    return stream
```

```python
import functools

import jax
import jax.numpy as jnp
from jax import lax
from jax.experimental import pallas as pl
from jax.experimental.pallas import tpu as pltpu
from jax.sharding import PartitionSpec as P

HALO = 32
ROWS = 32


def module_kernel(
    reach, first_ref, x_ref, gain_ref, wv_ref, wg_ref, wo_ref, taps_ref, lng_ref, lnb_ref,
    out_ref, hid_ref, glu_ref, fil_ref, norm_ref,
):
    step = pl.program_id(0)
    parts, rows_in, width = x_ref.shape
    rows = rows_in - HALO
    wide = glu_ref.shape[1]
    blocks = fil_ref.shape[0]

    @pl.when(step == 0)
    def _():
        total = jnp.zeros((rows_in, 1), jnp.float32)
        for q in range(parts):
            xf = x_ref[q].astype(jnp.float32)
            total = total + jnp.sum(xf * xf, axis=1, keepdims=True)
        scale = lax.rsqrt(total / (parts * width) + 1e-06)
        for q in range(parts):
            cols = slice(q * width, (q + 1) * width)
            xf = x_ref[q].astype(jnp.float32)
            hid_ref[:, cols] = (xf * scale * gain_ref[:, cols]).astype(jnp.bfloat16)

    @pl.when(step < blocks)
    def _():
        hidden = hid_ref[...]
        depth = hidden.shape[1]
        value = jnp.dot(hidden, wv_ref[...].reshape(depth, wide), preferred_element_type=jnp.float32)
        gate = jnp.dot(hidden, wg_ref[...].reshape(depth, wide), preferred_element_type=jnp.float32)
        glu = (value * jax.nn.sigmoid(gate)).astype(jnp.bfloat16).astype(jnp.float32)
        row = lax.broadcasted_iota(jnp.int32, (rows_in, 1), 0)
        glu_ref[...] = jnp.where(row < first_ref[0], 0.0, glu)
        lead = HALO - reach
        for r in range(0, rows, ROWS):
            acc = jnp.zeros((ROWS, wide), jnp.float32)
            for tap in range(reach + 1):
                acc = acc + taps_ref[0, tap : tap + 1, :] * glu_ref[pl.ds(r + lead + tap, ROWS), :]
            fil_ref[step, pl.ds(r, ROWS), :] = acc

    @pl.when(step == blocks)
    def _():
        channels = blocks * wide
        total = jnp.zeros((rows, 1), jnp.float32)
        square = jnp.zeros((rows, 1), jnp.float32)
        for b in range(blocks):
            f = fil_ref[b]
            total = total + jnp.sum(f, axis=1, keepdims=True)
            square = square + jnp.sum(f * f, axis=1, keepdims=True)
        mean = total / channels
        scale = lax.rsqrt(square / channels - mean * mean + 1e-06)
        for b in range(blocks):
            cols = slice(b * wide, (b + 1) * wide)
            v = (fil_ref[b] - mean) * scale * lng_ref[:, cols] + lnb_ref[:, cols]
            norm_ref[:, cols] = (v * jax.nn.sigmoid(v)).astype(jnp.bfloat16)

    @pl.when(step >= blocks)
    def _():
        acc = jnp.zeros((rows, width), jnp.float32)
        for b in range(blocks):
            acc = acc + lax.dot_general(
                norm_ref[:, b * wide : (b + 1) * wide],
                wo_ref[b].reshape(width, wide),
                (((1,), (1,)), ((), ())),
                preferred_element_type=jnp.float32,
            )
        kept = x_ref[step - blocks, HALO:, :].astype(jnp.float32)
        out_ref[0] = (kept + acc).astype(jnp.bfloat16)


def module(first, x, gain, weights, layer, taps, ln_gain, ln_bias):
    parts, rows_in, width = x.shape
    rows = rows_in - HALO
    blocks, shards, kinds, depth, wide = weights.shape
    reach = taps.shape[0] - 1
    taps = taps.reshape(reach + 1, blocks, wide).transpose(1, 0, 2)
    kind = 3 * layer
    group = shards // parts
    ahead = lambda i: jnp.minimum(i, blocks - 1)
    after = lambda i: jnp.maximum(i - blocks, 0)
    whole = lambda *shape: pl.BlockSpec(shape, lambda i: (0,) * len(shape))
    return pl.pallas_call(
        functools.partial(module_kernel, reach),
        grid=(blocks + parts,),
        in_specs=[
            pl.BlockSpec(memory_space=pltpu.SMEM),
            whole(parts, rows_in, width),
            whole(1, parts * width),
            pl.BlockSpec((None, shards, None, depth, wide), lambda i: (ahead(i), 0, kind, 0, 0)),
            pl.BlockSpec((None, shards, None, depth, wide), lambda i: (ahead(i), 0, kind + 1, 0, 0)),
            pl.BlockSpec((blocks, group, None, depth, wide), lambda i: (0, after(i), kind + 2, 0, 0)),
            pl.BlockSpec((1, reach + 1, wide), lambda i: (ahead(i), 0, 0)),
            whole(1, blocks * wide),
            whole(1, blocks * wide),
        ],
        out_specs=pl.BlockSpec((1, rows, width), lambda i: (after(i), 0, 0)),
        out_shape=jax.ShapeDtypeStruct((parts, rows, width), jnp.bfloat16),
        scratch_shapes=[
            pltpu.VMEM((rows_in, parts * width), jnp.bfloat16),
            pltpu.VMEM((rows_in, wide), jnp.float32),
            pltpu.VMEM((blocks, rows, wide), jnp.float32),
            pltpu.VMEM((rows, blocks * wide), jnp.bfloat16),
        ],
        compiler_params=pltpu.CompilerParams(dimension_semantics=("arbitrary",)),
        name=f"module_{layer}",
    )(first, x, gain[None], weights, weights, weights, taps, ln_gain[None], ln_bias[None])


def shards(inputs, norm_gain, w_value, w_gate, conv_taps, ln_gain, ln_bias, w_out):
    layers = norm_gain.shape[0]
    sp, tp = lax.axis_size("sp"), lax.axis_size("tp")
    rows = inputs.shape[0] // tp
    lead = layers * HALO
    kinds = jnp.stack((w_value, w_gate, jnp.swapaxes(w_out, 1, 2)), axis=1)
    depth, wide = kinds.shape[2:]
    packed = kinds.reshape(-1, wide)
    weights = lax.all_gather(packed, ("tp", "sp"), axis=0, tiled=True)
    weights = weights.reshape(tp, sp, 3 * layers, depth, wide)
    before = lax.ppermute(inputs[-lead:], "sp", [(i, i + 1) for i in range(sp - 1)])
    padded = jnp.concatenate((before, inputs), axis=0)
    windows = jnp.stack([padded[k * rows : (k + 1) * rows + lead] for k in range(tp)])
    x = lax.all_to_all(windows, "tp", 0, 0, tiled=True)
    start = (lax.axis_index("sp") * tp + lax.axis_index("tp")) * rows
    small = lax.all_gather(
        jnp.concatenate((conv_taps, ln_gain[:, None], ln_bias[:, None]), axis=1), "tp", axis=2, tiled=True
    )
    for layer in range(layers):
        first = jnp.maximum((layers - layer) * HALO - start, 0).astype(jnp.int32)[None]
        x = module(
            first, x, norm_gain[layer], weights, layer,
            small[layer, :-2], small[layer, -2], small[layer, -1],
        )
    return lax.all_to_all(x, "tp", 0, 0, tiled=True).reshape(inputs.shape)


def solution(mesh):
    in_specs = (
        P("sp", "tp"),
        P(),
        P(None, "sp", "tp"),
        P(None, "sp", "tp"),
        P(None, None, "tp"),
        P(None, "tp"),
        P(None, "tp"),
        P(None, "tp", "sp"),
    )
    out_specs = P("sp", "tp")
    return jax.shard_map(shards, mesh=mesh, in_specs=in_specs, out_specs=out_specs, check_vma=False)
```

```python
import functools

import jax
import jax.numpy as jnp
from jax import lax
from jax.experimental import pallas as pl
from jax.experimental.pallas import tpu as pltpu
from jax.sharding import Mesh, PartitionSpec as P


NZ, NX, NC, NY = 8, 4, 2, 4
HALO = 32
ROWS = 32
DEPTH, WIDE = 32, 256
GROUP = NX * NC * DEPTH
SPAN = {"z": NZ, "x": NX, "y": NY}

PLANS = (
    dict(last="x", outer="y", inner="z"),
    dict(last="y", outer="x", inner="z"),
    dict(last="z", outer="y", inner="x"),
)


def part_labels(last):
    span = SPAN[last]
    around = [(d, None) for d in range(span) if d != span // 2] + [(span // 2, 0), (span // 2, 1)]
    return [(d, half, c) for c in range(NC) for d, half in around]


def swap_cores(v, core):
    lane = lax.broadcasted_iota(jnp.int32, v.shape, 1)
    other = jnp.where(
        lane % (2 * DEPTH) < DEPTH,
        pltpu.roll(v, GROUP - DEPTH, 1),
        pltpu.roll(v, DEPTH, 1),
    )
    return jnp.where(core == 1, other, v)


def to_relative(v, at_x, core):
    return swap_cores(pltpu.roll(v, (NX - at_x) * (NC * DEPTH), 1), core)


def to_absolute(v, at_x, core):
    return pltpu.roll(swap_cores(v, core), at_x * (NC * DEPTH), 1)


def prepare_kernel(info_ref, before_ref, x_ref, gain_ref, windows_ref, rel_ref, pad_ref):
    at_z, at_x, core = info_ref[1], info_ref[2], info_ref[3]
    lead = before_ref.shape[0]
    count, halves, window, group = windows_ref.shape
    rows = window - lead
    for half in range(halves):
        cols = slice(half * group, (half + 1) * group)
        pad_ref[:lead] = to_relative(before_ref[:, cols].astype(jnp.float32), at_x, core).astype(jnp.bfloat16)
        for k in range(count):
            turned = to_relative(x_ref[k * rows : (k + 1) * rows, cols].astype(jnp.float32), at_x, core)
            pad_ref[lead + k * rows : lead + (k + 1) * rows] = turned.astype(jnp.bfloat16)
        for k in range(count):
            windows_ref[k, half] = pad_ref[k * rows : k * rows + window]
    for layer in range(gain_ref.shape[0]):
        for d in range(NZ):
            row = gain_ref[layer, pl.ds((at_z + d) % NZ, 1), :]
            rel_ref[layer, d : d + 1, :] = to_relative(jnp.broadcast_to(row, (8, group)), at_x, core)[:1]


def prepare(info, before, x, gain):
    lead, width = before.shape
    rows = x.shape[0] // NY
    return pl.pallas_call(
        prepare_kernel,
        in_specs=[pl.BlockSpec(memory_space=pltpu.SMEM)] + [pl.BlockSpec(memory_space=pltpu.VMEM)] * 3,
        out_specs=[pl.BlockSpec(memory_space=pltpu.VMEM)] * 2,
        out_shape=[
            jax.ShapeDtypeStruct((NY, width // GROUP, rows + lead, GROUP), jnp.bfloat16),
            jax.ShapeDtypeStruct((gain.shape[0], NZ, GROUP), jnp.float32),
        ],
        scratch_shapes=[pltpu.VMEM((lead + x.shape[0], GROUP), jnp.bfloat16)],
        name="prepare",
    )(info, before, x, gain.reshape(-1, NZ, GROUP))


def module_kernel(layer, layers, reach, n_parts, *refs):
    info_ref, x_ref, gain_ref, small_ref = refs[:4]
    part_refs, (out_ref, *refs) = refs[4 : 4 + n_parts], refs[4 + n_parts :]
    hid_ref, glu_ref, fil_ref, norm_ref, sems, *held = refs
    plan = PLANS[layer]
    last, outer, inner = plan["last"], plan["outer"], plan["inner"]
    labels = part_labels(last)
    rows_in = x_ref.shape[1]
    rows = rows_in - HALO
    channels = NY * WIDE
    at_z = info_ref[1] if layer == 0 else 0
    z_of = (lambda d: (at_z + d) % NZ) if layer == 0 else (lambda d: d)

    copies = [[] for _ in range(NY)]
    n = 0
    for dy in range(NY):
        for i, (d, half, _) in enumerate(labels):
            span = held[i].shape[0]
            if last == "y":
                if d != dy:
                    continue
                pieces = [(part_refs[i], held[i])]
            else:
                at = dy - (half or 0) * span
                if not 0 <= at < span:
                    continue
                pieces = [(part_refs[i].at[at], held[i].at[at])]
            for source, target in pieces:
                copies[dy].append(pltpu.make_async_copy(source, target, sems.at[n]))
                n += 1
    for group in copies:
        for copy in group:
            copy.start()

    def shard(kind, dy, dz, dx, dc):
        at = dict(x=dx, y=dy, z=dz)
        for i, (d, half, c) in enumerate(labels):
            span = held[i].shape[0]
            a = at[outer] - (half or 0) * span
            if d == at[last] and c == dc and 0 <= a < span:
                return held[i][a, at[inner], kind * DEPTH : (kind + 1) * DEPTH, :]

    def matrix(kind, dy, zs):
        return jnp.concatenate(
            [shard(kind, dy, dz, dx, dc) for dz in zs for dx in range(NX) for dc in range(NC)], axis=0
        )

    total = jnp.zeros((rows_in, 1), jnp.float32)
    for dz in range(NZ):
        xf = x_ref[dz].astype(jnp.float32)
        total = total + jnp.sum(xf * xf, axis=1, keepdims=True)
    scale = lax.rsqrt(total / (NZ * GROUP) + 1e-06)
    for dz in range(NZ):
        xf = x_ref[z_of(dz)].astype(jnp.float32)
        hid_ref[:, dz * GROUP : (dz + 1) * GROUP] = (xf * scale * gain_ref[layer, dz : dz + 1, :]).astype(jnp.bfloat16)

    lead = HALO - reach
    row = lax.broadcasted_iota(jnp.int32, (rows_in, 1), 0)
    ahead = row < info_ref[4 + layer]
    for dy in range(NY):
        for copy in copies[dy]:
            copy.wait()
        hidden = hid_ref[...]
        value = jnp.dot(hidden, matrix(0, dy, range(NZ)), preferred_element_type=jnp.float32)
        gate = jnp.dot(hidden, matrix(1, dy, range(NZ)), preferred_element_type=jnp.float32)
        glu = (value * jax.nn.sigmoid(gate)).astype(jnp.bfloat16).astype(jnp.float32)
        glu_ref[dy] = jnp.where(ahead, 0.0, glu)

    def filtered(dy, carry):
        for r in range(0, rows, ROWS):
            acc = jnp.zeros((ROWS, WIDE), jnp.float32)
            for tap in range(reach + 1):
                acc = acc + small_ref[dy, layer, tap : tap + 1, :] * glu_ref[dy, pl.ds(r + lead + tap, ROWS), :]
            fil_ref[dy, pl.ds(r, ROWS), :] = acc
        return carry

    lax.fori_loop(0, NY, filtered, 0)

    total = jnp.zeros((rows, 1), jnp.float32)
    square = jnp.zeros((rows, 1), jnp.float32)
    for dy in range(NY):
        f = fil_ref[dy]
        total = total + jnp.sum(f, axis=1, keepdims=True)
        square = square + jnp.sum(f * f, axis=1, keepdims=True)
    mean = total / channels
    scale = lax.rsqrt(square / channels - mean * mean + 1e-06)
    for dy in range(NY):
        gain = small_ref[dy, layer, reach + 1 : reach + 2, :]
        bias = small_ref[dy, layer, reach + 2 : reach + 3, :]
        v = (fil_ref[dy] - mean) * scale * gain + bias
        norm_ref[:, dy * WIDE : (dy + 1) * WIDE] = (v * jax.nn.sigmoid(v)).astype(jnp.bfloat16)

    for dz in range(NZ):
        acc = jnp.zeros((rows, GROUP), jnp.float32)
        for dy in range(NY):
            acc = acc + lax.dot_general(
                norm_ref[:, dy * WIDE : (dy + 1) * WIDE],
                matrix(2, dy, (dz,)),
                (((1,), (1,)), ((), ())),
                preferred_element_type=jnp.float32,
            )
        new = x_ref[z_of(dz), HALO:, :].astype(jnp.float32) + acc
        if layer < layers - 1:
            out_ref[dz] = new.astype(jnp.bfloat16)
        else:
            z = (info_ref[1] + dz) % NZ
            turned = to_absolute(new, info_ref[2], info_ref[3])
            at = pl.multiple_of((z % 2) * GROUP, GROUP)
            out_ref[z // 2, :, pl.ds(at, GROUP)] = turned.astype(jnp.bfloat16)


def module(info, x, gain, small, parts, layer, layers):
    rows_in = x.shape[1]
    rows = rows_in - HALO
    reach = small.shape[2] - 3
    vmem = pl.BlockSpec(memory_space=pltpu.VMEM)
    out = (NZ, rows, GROUP) if layer < layers - 1 else (NZ // 2, rows, 2 * GROUP)
    n_copies = sum(1 if PLANS[layer]["last"] == "y" else p.shape[0] for p in parts)
    return pl.pallas_call(
        functools.partial(module_kernel, layer, layers, reach, len(parts)),
        in_specs=[pl.BlockSpec(memory_space=pltpu.SMEM)] + [vmem] * 3
        + [pl.BlockSpec(memory_space=pl.ANY)] * len(parts),
        out_specs=vmem,
        out_shape=jax.ShapeDtypeStruct(out, jnp.bfloat16),
        scratch_shapes=[
            pltpu.VMEM((rows_in, NZ * GROUP), jnp.bfloat16),
            pltpu.VMEM((NY, rows_in, WIDE), jnp.float32),
            pltpu.VMEM((NY, rows, WIDE), jnp.float32),
            pltpu.VMEM((rows, NY * WIDE), jnp.bfloat16),
            pltpu.SemaphoreType.DMA((n_copies,)),
        ]
        + [pltpu.VMEM(p.shape, p.dtype) for p in parts],
        name=f"module_{layer}",
    )(info, x, gain, small, *parts)


def shift(a, axis, by):
    n = SPAN[axis]
    return lax.ppermute(a, axis, [(i, (i + by) % n) for i in range(n)])


def ring(block, axis):
    n = SPAN[axis]
    held = {0: block}
    up = down = block
    for k in range(1, n // 2):
        up, down = shift(up, axis, 1), shift(down, axis, -1)
        held[n - k], held[k] = up, down
    half = block.shape[0] // 2
    farthest = (shift(up[:half], axis, 1), shift(down[half:], axis, -1))
    return held, farthest


def gathered(block, axis):
    held, farthest = ring(block, axis)
    held[SPAN[axis] // 2] = jnp.concatenate(farthest)
    return [held[d] for d in range(SPAN[axis])]


def last_parts(block, axis):
    held, farthest = ring(block, axis)
    own = [held[d] for d in range(SPAN[axis]) if d in held] + list(farthest)
    return own + [lax.ppermute(p, "c", [(0, 1), (1, 0)]) for p in own]


def shards(inputs, norm_gain, w_value, w_gate, conv_taps, ln_gain, ln_bias, w_out):
    layers = norm_gain.shape[0]
    rows = inputs.shape[0] // NY
    lead = layers * HALO
    at_z, at_x, core, at_y = (lax.axis_index(a) for a in ("z", "x", "c", "y"))
    at = ((at_z * NX + at_x) * NC + core) * NY + at_y
    firsts = [jnp.maximum((layers - k) * HALO - at * rows, 0) for k in range(layers)]
    info = jnp.stack([at, at_z, at_x, core, *firsts]).astype(jnp.int32)
    sp = NZ * NX * NC
    before = lax.ppermute(inputs[-lead:], ("z", "x", "c"), [(i, i + 1) for i in range(sp - 1)])
    windows, gain = prepare(info, before, inputs, norm_gain)
    x = lax.all_to_all(windows, "y", 0, 0, tiled=True).reshape(NZ, rows + lead, GROUP)
    packed = jnp.concatenate((w_value, w_gate, jnp.swapaxes(w_out, 1, 2)), axis=1)
    first = gathered(packed[:2], "z")
    zs = [jnp.stack([p[k] for p in first]) for k in range(2)]
    block0 = jnp.stack(gathered(zs[0], "y"))
    block1 = jnp.stack(gathered(zs[1], "x"))
    alone = packed[2]
    xs = jnp.stack([alone, shift(alone, "x", -1), shift(alone, "x", 2), shift(alone, "x", 1)])
    block2 = jnp.stack(gathered(xs, "y"))
    parts = [last_parts(b, PLANS[k]["last"]) for k, b in enumerate((block0, block1, block2))]
    own = jnp.concatenate((conv_taps, ln_gain[:, None], ln_bias[:, None]), axis=1)
    small = jnp.stack([own, shift(own, "y", -1), shift(own, "y", 2), shift(own, "y", 1)])
    for layer in range(layers):
        x = module(info, x, gain, small, parts[layer], layer, layers)
    return lax.all_to_all(x, "y", 0, 0, tiled=True).reshape(inputs.shape)


def solution(mesh):
    mesh = Mesh(mesh.devices.reshape(NZ, NX, NC, NY), ("z", "x", "c", "y"))
    sp = ("z", "x", "c")
    in_specs = (
        P(sp, "y"),
        P(),
        P(None, sp, "y"),
        P(None, sp, "y"),
        P(None, None, "y"),
        P(None, "y"),
        P(None, "y"),
        P(None, "y", sp),
    )
    out_specs = P(sp, "y")
    return jax.shard_map(shards, mesh=mesh, in_specs=in_specs, out_specs=out_specs, check_vma=False)
```

```python
import functools

import jax
import jax.numpy as jnp
from jax import lax
from jax.experimental import pallas as pl
from jax.experimental.pallas import tpu as pltpu
from jax.sharding import Mesh, PartitionSpec as P


NZ, NX, NC, NY = 8, 4, 2, 4
HALO = 32
ROWS = 64
TILE = 8
DEPTH, WIDE = 32, 256
GROUP = NX * NC * DEPTH
SPAN = {"z": NZ, "x": NX, "y": NY}

PLANS = (
    dict(last="x", outer="y", inner="z"),
    dict(last="y", outer="x", inner="z"),
    dict(last="z", outer="y", inner="x"),
)


def part_labels(last):
    span = SPAN[last]
    around = [(d, None) for d in range(span) if d != span // 2] + [(span // 2, 0), (span // 2, 1)]
    return [(d, half, c) for c in range(NC) for d, half in around]


def swap_cores(v, core):
    lane = lax.broadcasted_iota(jnp.int32, v.shape, 1)
    other = jnp.where(
        lane % (2 * DEPTH) < DEPTH,
        pltpu.roll(v, GROUP - DEPTH, 1),
        pltpu.roll(v, DEPTH, 1),
    )
    return jnp.where(core == 1, other, v)


def to_relative(v, at_x, core):
    return swap_cores(pltpu.roll(v, (NX - at_x) * (NC * DEPTH), 1), core)


def to_absolute(v, at_x, core):
    return pltpu.roll(swap_cores(v, core), at_x * (NC * DEPTH), 1)


def prepare_kernel(info_ref, before_ref, x_ref, gain_ref, windows_ref, rel_ref, pad_ref):
    at_z, at_x, core = info_ref[1], info_ref[2], info_ref[3]
    lead = before_ref.shape[0]
    count, halves, window, group = windows_ref.shape
    rows = window - lead
    for half in range(halves):
        cols = slice(half * group, (half + 1) * group)
        pad_ref[:lead] = to_relative(before_ref[:, cols].astype(jnp.float32), at_x, core).astype(jnp.bfloat16)
        for k in range(count):
            turned = to_relative(x_ref[k * rows : (k + 1) * rows, cols].astype(jnp.float32), at_x, core)
            pad_ref[lead + k * rows : lead + (k + 1) * rows] = turned.astype(jnp.bfloat16)
        for k in range(count):
            windows_ref[k, half] = pad_ref[k * rows : k * rows + window]
    for layer in range(gain_ref.shape[0]):
        for d in range(NZ):
            row = gain_ref[layer, pl.ds((at_z + d) % NZ, 1), :]
            rel_ref[layer, d : d + 1, :] = to_relative(jnp.broadcast_to(row, (8, group)), at_x, core)[:1]


def prepare(info, before, x, gain):
    lead, width = before.shape
    rows = x.shape[0] // NY
    return pl.pallas_call(
        prepare_kernel,
        in_specs=[pl.BlockSpec(memory_space=pltpu.SMEM)] + [pl.BlockSpec(memory_space=pltpu.VMEM)] * 3,
        out_specs=[pl.BlockSpec(memory_space=pltpu.VMEM)] * 2,
        out_shape=[
            jax.ShapeDtypeStruct((NY, width // GROUP, rows + lead, GROUP), jnp.bfloat16),
            jax.ShapeDtypeStruct((gain.shape[0], NZ, GROUP), jnp.float32),
        ],
        scratch_shapes=[pltpu.VMEM((lead + x.shape[0], GROUP), jnp.bfloat16)],
        name="prepare",
    )(info, before, x, gain.reshape(-1, NZ, GROUP))


def module_kernel(layer, layers, reach, n_parts, *refs):
    info_ref, x_ref, gain_ref, small_ref = refs[:4]
    part_refs, (out_ref, *refs) = refs[4 : 4 + n_parts], refs[4 + n_parts :]
    hid_ref, glu_ref, fil_ref, norm_ref, held_ref, sems = refs
    plan = PLANS[layer]
    last, outer, inner = plan["last"], plan["outer"], plan["inner"]
    labels = part_labels(last)
    rows_in = x_ref.shape[1]
    rows = rows_in - HALO
    channels = NY * WIDE
    at_z = info_ref[1] if layer == 0 else 0
    z_of = (lambda d: (at_z + d) % NZ) if layer == 0 else (lambda d: d)

    copies = [[] for _ in range(NY)]
    n = 0
    for dy in range(NY):
        for i, (d, half, c) in enumerate(labels):
            span = part_refs[i].shape[0]
            low = (half or 0) * span
            if last == "y" and d == dy:
                pair = part_refs[i], held_ref.at[d, c, low : low + span]
            elif last != "y" and low <= dy < low + span:
                pair = part_refs[i].at[dy - low], held_ref.at[d, c, dy]
            else:
                continue
            copies[dy].append(pltpu.make_async_copy(*pair, sems.at[n]))
            n += 1
    for group in copies:
        for copy in group:
            copy.start()

    def shard(kind, dy, dz, dx, dc):
        at = dict(x=dx, y=dy, z=dz)
        return held_ref[at[last], dc, at[outer], at[inner], kind * DEPTH : (kind + 1) * DEPTH, :]

    def matrix(kind, dy, zs):
        return jnp.concatenate(
            [shard(kind, dy, dz, dx, dc) for dz in zs for dx in range(NX) for dc in range(NC)], axis=0
        )

    total = jnp.zeros((rows_in, 1), jnp.float32)
    for dz in range(NZ):
        xf = x_ref[dz].astype(jnp.float32)
        total = total + jnp.sum(xf * xf, axis=1, keepdims=True)
    scale = lax.rsqrt(total / (NZ * GROUP) + 1e-06)
    for dz in range(NZ):
        xf = x_ref[z_of(dz)].astype(jnp.float32)
        hid_ref[:, dz * GROUP : (dz + 1) * GROUP] = (xf * scale * gain_ref[layer, dz : dz + 1, :]).astype(jnp.bfloat16)

    lead = HALO - reach
    row = lax.broadcasted_iota(jnp.int32, (rows_in, 1), 0)
    ahead = row < info_ref[4 + layer]

    def block(dy, carry):
        for k in range(NY):

            @pl.when(dy == k)
            def _():
                for copy in copies[k]:
                    copy.wait()

        hidden = hid_ref[...]
        value = jnp.dot(hidden, matrix(0, dy, range(NZ)), preferred_element_type=jnp.float32)
        gate = jnp.dot(hidden, matrix(1, dy, range(NZ)), preferred_element_type=jnp.float32)
        glu = (value * jax.nn.sigmoid(gate)).astype(jnp.bfloat16).astype(jnp.float32)
        glu_ref[...] = jnp.where(ahead, 0.0, glu)
        for r in range(0, rows, ROWS):
            count = min(ROWS, rows - r)
            acc = jnp.zeros((count, WIDE), jnp.float32)
            for s in range(TILE):
                extra = TILE if s else 0
                part = jnp.zeros((count + extra, WIDE), jnp.float32)
                for tap in range(reach + 1):
                    if (tap + lead) % TILE == s:
                        at = r + tap + lead - s
                        part = part + small_ref[dy, layer, tap : tap + 1, :] * glu_ref[at : at + count + extra, :]
                acc = acc + part[s : s + count]
            fil_ref[dy, r : r + count, :] = acc
        return carry

    lax.fori_loop(0, NY, block, 0)

    total = jnp.zeros((rows, 1), jnp.float32)
    square = jnp.zeros((rows, 1), jnp.float32)
    for dy in range(NY):
        f = fil_ref[dy]
        total = total + jnp.sum(f, axis=1, keepdims=True)
        square = square + jnp.sum(f * f, axis=1, keepdims=True)
    mean = total / channels
    scale = lax.rsqrt(square / channels - mean * mean + 1e-06)
    for dy in range(NY):
        gain = small_ref[dy, layer, reach + 1 : reach + 2, :]
        bias = small_ref[dy, layer, reach + 2 : reach + 3, :]
        v = (fil_ref[dy] - mean) * scale * gain + bias
        norm_ref[:, dy * WIDE : (dy + 1) * WIDE] = (v * jax.nn.sigmoid(v)).astype(jnp.bfloat16)

    def features(dz, carry):
        weight = jnp.concatenate([matrix(2, dy, (dz,)) for dy in range(NY)], axis=1)
        acc = lax.dot_general(
            norm_ref[...], weight, (((1,), (1,)), ((), ())), preferred_element_type=jnp.float32
        )
        new = x_ref[z_of(dz), HALO:, :].astype(jnp.float32) + acc
        if layer < layers - 1:
            out_ref[dz] = new.astype(jnp.bfloat16)
        else:
            z = (info_ref[1] + dz) % NZ
            turned = to_absolute(new, info_ref[2], info_ref[3])
            at = pl.multiple_of((z % 2) * GROUP, GROUP)
            out_ref[z // 2, :, pl.ds(at, GROUP)] = turned.astype(jnp.bfloat16)
        return carry

    lax.fori_loop(0, NZ, features, 0)


def module(info, x, gain, small, parts, layer, layers):
    rows_in = x.shape[1]
    rows = rows_in - HALO
    reach = small.shape[2] - 3
    vmem = pl.BlockSpec(memory_space=pltpu.VMEM)
    out = (NZ, rows, GROUP) if layer < layers - 1 else (NZ // 2, rows, 2 * GROUP)
    plan = PLANS[layer]
    n_copies = sum(1 if plan["last"] == "y" else p.shape[0] for p in parts)
    return pl.pallas_call(
        functools.partial(module_kernel, layer, layers, reach, len(parts)),
        in_specs=[pl.BlockSpec(memory_space=pltpu.SMEM)] + [vmem] * 3
        + [pl.BlockSpec(memory_space=pl.ANY)] * len(parts),
        out_specs=vmem,
        out_shape=jax.ShapeDtypeStruct(out, jnp.bfloat16),
        scratch_shapes=[
            pltpu.VMEM((rows_in, NZ * GROUP), jnp.bfloat16),
            pltpu.VMEM((rows_in, WIDE), jnp.float32),
            pltpu.VMEM((NY, rows, WIDE), jnp.float32),
            pltpu.VMEM((rows, NY * WIDE), jnp.bfloat16),
            pltpu.VMEM((SPAN[plan["last"]], NC, SPAN[plan["outer"]], SPAN[plan["inner"]], 3 * DEPTH, WIDE), jnp.bfloat16),
            pltpu.SemaphoreType.DMA((n_copies,)),
        ],
        cost_estimate=pl.CostEstimate(
            flops=6 * rows_in * NZ * GROUP * NY * WIDE, transcendentals=0, bytes_accessed=6 * NZ * GROUP * NY * WIDE
        ),
        name=f"module_{layer}",
    )(info, x, gain, small, *parts)


def shift(a, axis, by):
    n = SPAN[axis]
    return lax.ppermute(a, axis, [(i, (i + by) % n) for i in range(n)])


def ring(block, axis):
    n = SPAN[axis]
    held = {0: block}
    up = down = block
    for k in range(1, n // 2):
        up, down = shift(up, axis, 1), shift(down, axis, -1)
        held[n - k], held[k] = up, down
    half = block.shape[0] // 2
    farthest = (shift(up[:half], axis, 1), shift(down[half:], axis, -1))
    return held, farthest


def gathered(block, axis):
    held, farthest = ring(block, axis)
    held[SPAN[axis] // 2] = jnp.concatenate(farthest)
    return [held[d] for d in range(SPAN[axis])]


def last_parts(block, axis):
    held, farthest = ring(block, axis)
    own = [held[d] for d in range(SPAN[axis]) if d in held] + list(farthest)
    return own + [lax.ppermute(p, "c", [(0, 1), (1, 0)]) for p in own]


def shards(inputs, norm_gain, w_value, w_gate, conv_taps, ln_gain, ln_bias, w_out):
    layers = norm_gain.shape[0]
    rows = inputs.shape[0] // NY
    lead = layers * HALO
    at_z, at_x, core, at_y = (lax.axis_index(a) for a in ("z", "x", "c", "y"))
    at = ((at_z * NX + at_x) * NC + core) * NY + at_y
    firsts = [jnp.maximum((layers - k) * HALO - at * rows, 0) for k in range(layers)]
    info = jnp.stack([at, at_z, at_x, core, *firsts]).astype(jnp.int32)
    sp = NZ * NX * NC
    before = lax.ppermute(inputs[-lead:], ("z", "x", "c"), [(i, i + 1) for i in range(sp - 1)])
    windows, gain = prepare(info, before, inputs, norm_gain)
    x = lax.all_to_all(windows, "y", 0, 0, tiled=True).reshape(NZ, rows + lead, GROUP)
    packed = jnp.concatenate((w_value, w_gate, jnp.swapaxes(w_out, 1, 2)), axis=1)
    first = [packed[:2]] + [shift(packed[:2], "z", -d) for d in range(1, NZ)]
    first, (windows, gain) = lax.optimization_barrier((first, (windows, gain)))
    zs = [jnp.stack([p[k] for p in first]) for k in range(2)]
    block0 = jnp.stack(gathered(zs[0], "y"))
    block1 = jnp.stack(gathered(zs[1], "x"))
    alone = packed[2]
    xs = jnp.stack([alone, shift(alone, "x", -1), shift(alone, "x", 2), shift(alone, "x", 1)])
    block2 = jnp.stack(gathered(xs, "y"))
    parts = [last_parts(b, PLANS[k]["last"]) for k, b in enumerate((block0, block1, block2))]
    own = jnp.concatenate((conv_taps, ln_gain[:, None], ln_bias[:, None]), axis=1)
    small = jnp.stack([own, shift(own, "y", -1), shift(own, "y", 2), shift(own, "y", 1)])
    for layer in range(layers):
        x = module(info, x, gain, small, parts[layer], layer, layers)
    return lax.all_to_all(x, "y", 0, 0, tiled=True).reshape(inputs.shape)


def solution(mesh):
    mesh = Mesh(mesh.devices.reshape(NZ, NX, NC, NY), ("z", "x", "c", "y"))
    sp = ("z", "x", "c")
    in_specs = (
        P(sp, "y"),
        P(),
        P(None, sp, "y"),
        P(None, sp, "y"),
        P(None, None, "y"),
        P(None, "y"),
        P(None, "y"),
        P(None, "y", sp),
    )
    out_specs = P(sp, "y")
    return jax.shard_map(shards, mesh=mesh, in_specs=in_specs, out_specs=out_specs, check_vma=False)
```

```python
import functools

import jax
import jax.numpy as jnp
from jax import lax
from jax.experimental import pallas as pl
from jax.experimental.pallas import tpu as pltpu
from jax.sharding import Mesh, PartitionSpec as P


NZ, NX, NC, NY = 8, 4, 2, 4
HALO = 32
ROWS = 64
TILE = 8
DEPTH, WIDE = 32, 256
GROUP = NX * NC * DEPTH
SPAN = {"z": NZ, "x": NX, "y": NY}

FIRST = dict(last="z", outer="y", inner="x")


def part_labels(last):
    span = SPAN[last]
    around = [(d, None) for d in range(span) if d != span // 2] + [(span // 2, 0), (span // 2, 1)]
    return [(d, half, c) for c in range(NC) for d, half in around]


def swap_cores(v, core):
    lane = lax.broadcasted_iota(jnp.int32, v.shape, 1)
    other = jnp.where(
        lane % (2 * DEPTH) < DEPTH,
        pltpu.roll(v, GROUP - DEPTH, 1),
        pltpu.roll(v, DEPTH, 1),
    )
    return jnp.where(core == 1, other, v)


def to_relative(v, at_x, core):
    return swap_cores(pltpu.roll(v, (NX - at_x) * (NC * DEPTH), 1), core)


def to_absolute(v, at_x, core):
    return pltpu.roll(swap_cores(v, core), at_x * (NC * DEPTH), 1)


def prepare_kernel(info_ref, before_ref, x_ref, gain_ref, windows_ref, rel_ref, pad_ref):
    at_z, at_x, core = info_ref[1], info_ref[2], info_ref[3]
    lead = before_ref.shape[0]
    count, halves, window, group = windows_ref.shape
    rows = window - lead
    for half in range(halves):
        cols = slice(half * group, (half + 1) * group)
        pad_ref[:lead] = to_relative(before_ref[:, cols].astype(jnp.float32), at_x, core).astype(jnp.bfloat16)
        for k in range(count):
            turned = to_relative(x_ref[k * rows : (k + 1) * rows, cols].astype(jnp.float32), at_x, core)
            pad_ref[lead + k * rows : lead + (k + 1) * rows] = turned.astype(jnp.bfloat16)
        for k in range(count):
            windows_ref[k, half] = pad_ref[k * rows : k * rows + window]
    for layer in range(gain_ref.shape[0]):
        for d in range(NZ):
            row = gain_ref[layer, pl.ds((at_z + d) % NZ, 1), :]
            rel_ref[layer, d : d + 1, :] = to_relative(jnp.broadcast_to(row, (8, group)), at_x, core)[:1]


def prepare(info, before, x, gain):
    lead, width = before.shape
    rows = x.shape[0] // NY
    return pl.pallas_call(
        prepare_kernel,
        in_specs=[pl.BlockSpec(memory_space=pltpu.SMEM)] + [pl.BlockSpec(memory_space=pltpu.VMEM)] * 3,
        out_specs=[pl.BlockSpec(memory_space=pltpu.VMEM)] * 2,
        out_shape=[
            jax.ShapeDtypeStruct((NY, width // GROUP, rows + lead, GROUP), jnp.bfloat16),
            jax.ShapeDtypeStruct((gain.shape[0], NZ, GROUP), jnp.float32),
        ],
        scratch_shapes=[pltpu.VMEM((lead + x.shape[0], GROUP), jnp.bfloat16)],
        name="prepare",
    )(info, before, x, gain.reshape(-1, NZ, GROUP))


def one_module(layer, reach, info_ref, x_of, gain_ref, small_of, shard, waits, store, hid_ref, glu_ref, fil_ref, norm_ref):
    rows_in = x_of(0).shape[0]
    rows = rows_in - HALO
    channels = NY * WIDE

    def matrix(kind, dy, zs):
        return jnp.concatenate(
            [shard(kind, dy, dz, dx, dc) for dz in zs for dx in range(NX) for dc in range(NC)], axis=0
        )

    total = jnp.zeros((rows_in, 1), jnp.float32)
    for dz in range(NZ):
        xf = x_of(dz).astype(jnp.float32)
        total = total + jnp.sum(xf * xf, axis=1, keepdims=True)
    scale = lax.rsqrt(total / (NZ * GROUP) + 1e-06)
    for dz in range(NZ):
        xf = x_of(dz).astype(jnp.float32)
        hid_ref[:rows_in, dz * GROUP : (dz + 1) * GROUP] = (xf * scale * gain_ref[layer, dz : dz + 1, :]).astype(
            jnp.bfloat16
        )

    lead = HALO - reach
    row = lax.broadcasted_iota(jnp.int32, (rows_in, 1), 0)
    ahead = row < info_ref[4 + layer]

    def block(dy, carry):
        for k in range(NY):

            @pl.when(dy == k)
            def _():
                for copy in waits[k]:
                    copy.wait()

        hidden = hid_ref[:rows_in]
        value = jnp.dot(hidden, matrix(0, dy, range(NZ)), preferred_element_type=jnp.float32)
        gate = jnp.dot(hidden, matrix(1, dy, range(NZ)), preferred_element_type=jnp.float32)
        glu = (value * jax.nn.sigmoid(gate)).astype(jnp.bfloat16).astype(jnp.float32)
        glu_ref[:rows_in] = jnp.where(ahead, 0.0, glu)
        for r in range(0, rows, ROWS):
            count = min(ROWS, rows - r)
            acc = jnp.zeros((count, WIDE), jnp.float32)
            for s in range(TILE):
                extra = TILE if s else 0
                part = jnp.zeros((count + extra, WIDE), jnp.float32)
                for tap in range(reach + 1):
                    if (tap + lead) % TILE == s:
                        at = r + tap + lead - s
                        part = part + small_of(dy, layer, tap) * glu_ref[at : at + count + extra, :]
                acc = acc + part[s : s + count]
            fil_ref[dy, r : r + count, :] = acc
        return carry

    lax.fori_loop(0, NY, block, 0)

    total = jnp.zeros((rows, 1), jnp.float32)
    square = jnp.zeros((rows, 1), jnp.float32)
    for dy in range(NY):
        f = fil_ref[dy, :rows]
        total = total + jnp.sum(f, axis=1, keepdims=True)
        square = square + jnp.sum(f * f, axis=1, keepdims=True)
    mean = total / channels
    scale = lax.rsqrt(square / channels - mean * mean + 1e-06)
    for dy in range(NY):
        v = (fil_ref[dy, :rows] - mean) * scale * small_of(dy, layer, reach + 1) + small_of(dy, layer, reach + 2)
        norm_ref[:rows, dy * WIDE : (dy + 1) * WIDE] = (v * jax.nn.sigmoid(v)).astype(jnp.bfloat16)

    def features(dz, carry):
        weight = jnp.concatenate([matrix(2, dy, (dz,)) for dy in range(NY)], axis=1)
        acc = lax.dot_general(
            norm_ref[:rows], weight, (((1,), (1,)), ((), ())), preferred_element_type=jnp.float32
        )
        store(dz, x_of(dz, HALO).astype(jnp.float32) + acc)
        return carry

    lax.fori_loop(0, NZ, features, 0)


def first_kernel(reach, n_parts, *refs):
    info_ref, x_ref, gain_ref, small_ref = refs[:4]
    part_refs, (out_ref, *work, held_ref, sems) = refs[4 : 4 + n_parts], refs[4 + n_parts :]
    at_z, at_x, core, at_y = info_ref[1], info_ref[2], info_ref[3], info_ref[7]

    copies = [[] for _ in range(NY)]
    n = 0
    for dy in range(NY):
        for i, (d, half, c) in enumerate(part_labels(FIRST["last"])):
            span = part_refs[i].shape[0]
            low = (half or 0) * span
            if low <= dy < low + span:
                copies[dy].append(
                    pltpu.make_async_copy(part_refs[i].at[dy - low], held_ref.at[d, c, dy], sems.at[n])
                )
                n += 1
    for group in copies:
        for copy in group:
            copy.start()

    def store(dz, new):
        out_ref[(at_z + dz) % NZ] = to_absolute(new, at_x, core).astype(jnp.bfloat16)

    one_module(
        0, reach, info_ref,
        lambda dz, skip=0: x_ref[(at_z + dz) % NZ, skip:, :],
        gain_ref,
        lambda dy, layer, i: small_ref[(at_y + dy) % NY, layer, i : i + 1, :],
        lambda kind, dy, dz, dx, dc: held_ref[dz, dc, dy, dx, kind * DEPTH : (kind + 1) * DEPTH, :],
        copies, store, *work,
    )


def later_kernel(layers, reach, info_ref, x_ref, gain_ref, small_ref, whole_ref, out_ref, *refs):
    *work, mid_ref, held_ref, sems = refs
    copies = {}
    for layer in range(1, layers):
        copies[layer] = [
            [pltpu.make_async_copy(whole_ref.at[dy, :, layer - 1], held_ref.at[layer - 1, dy], sems.at[layer - 1, dy])]
            for dy in range(NY)
        ]
    for group in copies.values():
        for (copy,) in group:
            copy.start()

    for layer in range(1, layers):
        source = x_ref if layer == 1 else mid_ref

        def store(dz, new, layer=layer):
            if layer < layers - 1:
                mid_ref[dz] = new.astype(jnp.bfloat16)
            else:
                at = pl.multiple_of((dz % 2) * GROUP, GROUP)
                out_ref[dz // 2, :, pl.ds(at, GROUP)] = new.astype(jnp.bfloat16)

        one_module(
            layer, reach, info_ref,
            lambda dz, skip=0, source=source: source[dz, skip:, :],
            gain_ref,
            lambda dy, layer, i: small_ref[dy, layer, i : i + 1, :],
            lambda kind, dy, dz, dx, dc, layer=layer: held_ref[
                layer - 1, dy, (dz * NX + dx) * NC + dc, kind * DEPTH : (kind + 1) * DEPTH, :
            ],
            copies[layer], store, *work,
        )


def work_space(rows_in):
    rows = rows_in - HALO
    return [
        pltpu.VMEM((rows_in, NZ * GROUP), jnp.bfloat16),
        pltpu.VMEM((rows_in, WIDE), jnp.float32),
        pltpu.VMEM((NY, rows, WIDE), jnp.float32),
        pltpu.VMEM((rows, NY * WIDE), jnp.bfloat16),
    ]


def first_module(info, x, gain, small, parts):
    rows_in = x.shape[1]
    vmem = pl.BlockSpec(memory_space=pltpu.VMEM)
    return pl.pallas_call(
        functools.partial(first_kernel, small.shape[2] - 3, len(parts)),
        in_specs=[pl.BlockSpec(memory_space=pltpu.SMEM)]
        + [vmem] * 3
        + [pl.BlockSpec(memory_space=pl.ANY)] * len(parts),
        out_specs=vmem,
        out_shape=jax.ShapeDtypeStruct((NZ, rows_in - HALO, GROUP), jnp.bfloat16),
        scratch_shapes=work_space(rows_in)
        + [
            pltpu.VMEM((NZ, NC, NY, NX, 3 * DEPTH, WIDE), jnp.bfloat16),
            pltpu.SemaphoreType.DMA((sum(p.shape[0] for p in parts),)),
        ],
        cost_estimate=pl.CostEstimate(flops=6 * rows_in * 2048 * 1024, transcendentals=0, bytes_accessed=6 * 2048 * 1024),
        name="first_module",
    )(info, x, gain, small, *parts)


def later_modules(info, x, gain, small, whole):
    rows_in = x.shape[1]
    layers = gain.shape[0]
    rows = rows_in - (layers - 1) * HALO
    vmem = pl.BlockSpec(memory_space=pltpu.VMEM)
    return pl.pallas_call(
        functools.partial(later_kernel, layers, small.shape[2] - 3),
        in_specs=[pl.BlockSpec(memory_space=pltpu.SMEM)] + [vmem] * 3 + [pl.BlockSpec(memory_space=pl.ANY)],
        out_specs=vmem,
        out_shape=jax.ShapeDtypeStruct((NZ // 2, rows, 2 * GROUP), jnp.bfloat16),
        scratch_shapes=work_space(rows_in)
        + [
            pltpu.VMEM((NZ, rows_in - HALO, GROUP), jnp.bfloat16),
            pltpu.VMEM((layers - 1, NY, NZ * NX * NC, 3 * DEPTH, WIDE), jnp.bfloat16),
            pltpu.SemaphoreType.DMA((layers - 1, NY)),
        ],
        name="later_modules",
    )(info, x, gain, small, whole)


def shift(a, axis, by):
    n = SPAN[axis]
    return lax.ppermute(a, axis, [(i, (i + by) % n) for i in range(n)])


def ring(block, axis):
    n = SPAN[axis]
    held = {0: block}
    up = down = block
    for k in range(1, n // 2):
        up, down = shift(up, axis, 1), shift(down, axis, -1)
        held[n - k], held[k] = up, down
    half = block.shape[0] // 2
    farthest = (shift(up[:half], axis, 1), shift(down[half:], axis, -1))
    return held, farthest


def gathered(block, axis):
    held, farthest = ring(block, axis)
    held[SPAN[axis] // 2] = jnp.concatenate(farthest)
    return [held[d] for d in range(SPAN[axis])]


def last_parts(block, axis):
    held, farthest = ring(block, axis)
    own = [held[d] for d in range(SPAN[axis]) if d in held] + list(farthest)
    return own + [lax.ppermute(p, "c", [(0, 1), (1, 0)]) for p in own]


def shards(inputs, norm_gain, w_value, w_gate, conv_taps, ln_gain, ln_bias, w_out):
    layers = norm_gain.shape[0]
    rows = inputs.shape[0] // NY
    lead = layers * HALO
    at_z, at_x, core, at_y = (lax.axis_index(a) for a in ("z", "x", "c", "y"))
    at = ((at_z * NX + at_x) * NC + core) * NY + at_y
    firsts = [jnp.maximum((layers - k) * HALO - at * rows, 0) for k in range(layers)]
    info = jnp.stack([at, at_z, at_x, core, *firsts, at_y]).astype(jnp.int32)
    sp = NZ * NX * NC
    before = lax.ppermute(inputs[-lead:], ("z", "x", "c"), [(i, i + 1) for i in range(sp - 1)])
    windows, gain = prepare(info, before, inputs, norm_gain)
    x = lax.all_to_all(windows, "y", 0, 0, tiled=True).reshape(NZ, rows + lead, GROUP)
    packed = jnp.concatenate((w_value, w_gate, jnp.swapaxes(w_out, 1, 2)), axis=1)
    later = packed[1:].reshape(-1, WIDE)
    whole = lax.all_gather(later, ("y", "z", "x", "c"), axis=0, tiled=True)
    whole = whole.reshape(NY, sp, layers - 1, 3 * DEPTH, WIDE)
    alone = packed[0]
    xs = jnp.stack([alone, shift(alone, "x", -1), shift(alone, "x", 2), shift(alone, "x", 1)])
    block0 = jnp.stack(gathered(xs, "y"))
    parts = last_parts(block0, "z")
    own = jnp.concatenate((conv_taps, ln_gain[:, None], ln_bias[:, None]), axis=1)
    small = lax.all_to_all(jnp.broadcast_to(own, (NY, *own.shape)), "y", 0, 0, tiled=True)
    x = first_module(info, x, gain, small, parts)
    x = later_modules(info, x, norm_gain.reshape(layers, NZ, GROUP), small, whole)
    return lax.all_to_all(x, "y", 0, 0, tiled=True).reshape(inputs.shape)


def solution(mesh):
    mesh = Mesh(mesh.devices.reshape(NZ, NX, NC, NY), ("z", "x", "c", "y"))
    sp = ("z", "x", "c")
    in_specs = (
        P(sp, "y"),
        P(),
        P(None, sp, "y"),
        P(None, sp, "y"),
        P(None, None, "y"),
        P(None, "y"),
        P(None, "y"),
        P(None, "y", sp),
    )
    out_specs = P(sp, "y")
    return jax.shard_map(shards, mesh=mesh, in_specs=in_specs, out_specs=out_specs, check_vma=False)
```

```python
import functools

import jax
import jax.numpy as jnp
from jax import lax
from jax.experimental import pallas as pl
from jax.experimental.pallas import tpu as pltpu
from jax.sharding import Mesh, PartitionSpec as P


NZ, NX, NC, NY = 8, 4, 2, 4
HALO = 32
ROWS = 64
TILE = 8
DEPTH, WIDE = 32, 256
GROUP = NX * NC * DEPTH
SPAN = {"z": NZ, "x": NX, "y": NY}

PLANS = (
    dict(last="z", outer="y", inner="x"),
    dict(last="y", outer="x", inner="z"),
    dict(last="x", outer="y", inner="z"),
)


def swap_cores(v, core):
    lane = lax.broadcasted_iota(jnp.int32, v.shape, 1)
    other = jnp.where(
        lane % (2 * DEPTH) < DEPTH,
        pltpu.roll(v, GROUP - DEPTH, 1),
        pltpu.roll(v, DEPTH, 1),
    )
    return jnp.where(core == 1, other, v)


def to_relative(v, at_x, core):
    return swap_cores(pltpu.roll(v, (NX - at_x) * (NC * DEPTH), 1), core)


def to_absolute(v, at_x, core):
    return pltpu.roll(swap_cores(v, core), at_x * (NC * DEPTH), 1)


def prepare_kernel(info_ref, before_ref, x_ref, gain_ref, windows_ref, rel_ref, pad_ref):
    at_z, at_x, core = info_ref[1], info_ref[2], info_ref[3]
    lead = before_ref.shape[0]
    count, halves, window, group = windows_ref.shape
    rows = window - lead
    for half in range(halves):
        cols = slice(half * group, (half + 1) * group)
        pad_ref[:lead] = to_relative(before_ref[:, cols].astype(jnp.float32), at_x, core).astype(jnp.bfloat16)
        for k in range(count):
            turned = to_relative(x_ref[k * rows : (k + 1) * rows, cols].astype(jnp.float32), at_x, core)
            pad_ref[lead + k * rows : lead + (k + 1) * rows] = turned.astype(jnp.bfloat16)
        for k in range(count):
            windows_ref[k, half] = pad_ref[k * rows : k * rows + window]
    for layer in range(gain_ref.shape[0]):
        for d in range(NZ):
            row = gain_ref[layer, pl.ds((at_z + d) % NZ, 1), :]
            rel_ref[layer, d : d + 1, :] = to_relative(jnp.broadcast_to(row, (8, group)), at_x, core)[:1]


def prepare(info, before, x, gain):
    lead, width = before.shape
    rows = x.shape[0] // NY
    return pl.pallas_call(
        prepare_kernel,
        in_specs=[pl.BlockSpec(memory_space=pltpu.SMEM)] + [pl.BlockSpec(memory_space=pltpu.VMEM)] * 3,
        out_specs=[pl.BlockSpec(memory_space=pltpu.VMEM)] * 2,
        out_shape=[
            jax.ShapeDtypeStruct((NY, width // GROUP, rows + lead, GROUP), jnp.bfloat16),
            jax.ShapeDtypeStruct((gain.shape[0], NZ, GROUP), jnp.float32),
        ],
        scratch_shapes=[pltpu.VMEM((lead + x.shape[0], GROUP), jnp.bfloat16)],
        name="prepare",
    )(info, before, x, gain.reshape(-1, NZ, GROUP))


def one_module(layer, reach, info_ref, x_of, gain_ref, small_of, shard, waits, starts, store, hid_ref, glu_ref, fil_ref, norm_ref):
    rows_in = x_of(0).shape[0]
    rows = rows_in - HALO
    channels = NY * WIDE

    def matrix(kind, dy, zs):
        return jnp.concatenate(
            [shard(kind, dy, dz, dx, dc) for dz in zs for dx in range(NX) for dc in range(NC)], axis=0
        )

    total = jnp.zeros((rows_in, 1), jnp.float32)
    for dz in range(NZ):
        xf = x_of(dz).astype(jnp.float32)
        total = total + jnp.sum(xf * xf, axis=1, keepdims=True)
    scale = lax.rsqrt(total / (NZ * GROUP) + 1e-06)
    for dz in range(NZ):
        xf = x_of(dz).astype(jnp.float32)
        hid_ref[:rows_in, dz * GROUP : (dz + 1) * GROUP] = (xf * scale * gain_ref[layer, dz : dz + 1, :]).astype(
            jnp.bfloat16
        )

    lead = HALO - reach
    row = lax.broadcasted_iota(jnp.int32, (rows_in, 1), 0)
    ahead = row < info_ref[4 + layer]

    def block(dy, carry):
        for k in range(NY):

            @pl.when(dy == k)
            def _():
                for copy in waits[k]:
                    copy.wait()
                for copy in starts[k]:
                    copy.start()

        hidden = hid_ref[:rows_in]
        value = jnp.dot(hidden, matrix(0, dy, range(NZ)), preferred_element_type=jnp.float32)
        gate = jnp.dot(hidden, matrix(1, dy, range(NZ)), preferred_element_type=jnp.float32)
        glu = (value * jax.nn.sigmoid(gate)).astype(jnp.bfloat16).astype(jnp.float32)
        glu_ref[:rows_in] = jnp.where(ahead, 0.0, glu)
        for r in range(0, rows, ROWS):
            count = min(ROWS, rows - r)
            acc = jnp.zeros((count, WIDE), jnp.float32)
            for s in range(TILE):
                extra = TILE if s else 0
                part = jnp.zeros((count + extra, WIDE), jnp.float32)
                for tap in range(reach + 1):
                    if (tap + lead) % TILE == s:
                        at = r + tap + lead - s
                        part = part + small_of(dy, layer, tap) * glu_ref[at : at + count + extra, :]
                acc = acc + part[s : s + count]
            fil_ref[dy, r : r + count, :] = acc
        return carry

    lax.fori_loop(0, NY, block, 0)

    total = jnp.zeros((rows, 1), jnp.float32)
    square = jnp.zeros((rows, 1), jnp.float32)
    for dy in range(NY):
        f = fil_ref[dy, :rows]
        total = total + jnp.sum(f, axis=1, keepdims=True)
        square = square + jnp.sum(f * f, axis=1, keepdims=True)
    mean = total / channels
    scale = lax.rsqrt(square / channels - mean * mean + 1e-06)
    for dy in range(NY):
        v = (fil_ref[dy, :rows] - mean) * scale * small_of(dy, layer, reach + 1) + small_of(dy, layer, reach + 2)
        norm_ref[:rows, dy * WIDE : (dy + 1) * WIDE] = (v * jax.nn.sigmoid(v)).astype(jnp.bfloat16)

    def features(dz, carry):
        weight = jnp.concatenate([matrix(2, dy, (dz,)) for dy in range(NY)], axis=1)
        acc = lax.dot_general(
            norm_ref[:rows], weight, (((1,), (1,)), ((), ())), preferred_element_type=jnp.float32
        )
        store(dz, x_of(dz, HALO).astype(jnp.float32) + acc)
        return carry

    lax.fori_loop(0, NZ, features, 0)


def copies_of(plan, part_refs, held_ref, core, sems):
    n = SPAN[plan["last"]]
    half = held_ref.shape[2] // 2
    pairs = [[(part_refs[0], held_ref.at[0, 0]), (part_refs[1], held_ref.at[0, 1])]]
    for k in range(1, n // 2 + 1):
        mine, other = part_refs[2 * k : 2 * k + 2]
        here = jnp.where(core == 0, n - k, k)
        there = n - here
        if k < n // 2:
            to = lambda d, c: held_ref.at[d, c]
        else:
            here, there = core, 1 - core
            to = lambda d, c, k=k: held_ref.at[k, c, pl.ds(d * half, half)]
        pairs.append(
            [(part.at[c], to(d, c ^ swap)) for part, d, swap in ((mine, here, 0), (other, there, 1)) for c in range(NC)]
        )
    if plan["last"] != "y":
        pairs = [[pair for group in pairs for pair in group]]
    count = iter(range(sems.shape[0]))
    copies = [[pltpu.make_async_copy(*pair, sems.at[next(count)]) for pair in group] for group in pairs]
    return copies + [[]] * (NY - len(copies))


def modules_kernel(first, counts, reach, *refs):
    (info_ref, x_ref, gain_ref, small_ref), refs = refs[:4], refs[4:]
    part_refs = []
    for n in counts:
        part_refs.append(refs[:n])
        refs = refs[n:]
    out_ref, *refs = refs
    work, (mid_ref, *refs) = refs[:4], refs[4:]
    held_refs, sems = refs[: len(counts)], refs[len(counts) :]
    at_z, at_x, core, at_y = info_ref[1], info_ref[2], info_ref[3], info_ref[7]

    copies = [
        copies_of(PLANS[first + k], part_refs[k], held_refs[k], core, sems[k]) for k in range(len(counts))
    ]
    for group in copies[0][:2]:
        for copy in group:
            copy.start()
    starts = [[*groups[2:], [], []] for groups in copies]
    for k, groups in enumerate(copies[1:]):
        starts[k][2] = [copy for group in groups[:2] for copy in group]

    for k in range(len(counts)):
        layer = first + k
        plan, held_ref = PLANS[layer], held_refs[k]
        source = x_ref if k == 0 else mid_ref

        def x_of(dz, skip=0, source=source, layer=layer):
            return source[(at_z + dz) % NZ if layer == 0 else dz, skip:, :]

        def shard(kind, dy, dz, dx, dc, plan=plan, held_ref=held_ref):
            at = dict(x=dx, y=dy, z=dz)
            place = at[plan["last"]], dc, at[plan["outer"]], at[plan["inner"]]
            return held_ref[(*place, slice(kind * DEPTH, (kind + 1) * DEPTH))]

        def store(dz, new, layer=layer, k=k):
            if k < len(counts) - 1:
                mid_ref[dz] = new.astype(jnp.bfloat16)
            elif layer < len(PLANS) - 1:
                out_ref[dz] = new.astype(jnp.bfloat16)
            else:
                z = (at_z + dz) % NZ
                at = pl.multiple_of((z % 2) * GROUP, GROUP)
                out_ref[z // 2, :, pl.ds(at, GROUP)] = to_absolute(new, at_x, core).astype(jnp.bfloat16)

        one_module(
            layer, reach, info_ref, x_of, gain_ref,
            lambda dy, layer, i: small_ref[(at_y + dy) % NY, layer, i : i + 1, :],
            shard, copies[k], starts[k], store, *work,
        )


def modules(info, x, gain, small, parts, first):
    rows_in = x.shape[1]
    rows = rows_in - len(parts) * HALO
    vmem = pl.BlockSpec(memory_space=pltpu.VMEM)
    last = first + len(parts) == len(PLANS)
    plans = PLANS[first : first + len(parts)]
    return pl.pallas_call(
        functools.partial(modules_kernel, first, [len(p) for p in parts], small.shape[2] - 3),
        in_specs=[pl.BlockSpec(memory_space=pltpu.SMEM)]
        + [vmem] * 3
        + [pl.BlockSpec(memory_space=pl.ANY)] * sum(len(p) for p in parts),
        out_specs=vmem,
        out_shape=jax.ShapeDtypeStruct((NZ // 2, rows, 2 * GROUP) if last else (NZ, rows, GROUP), jnp.bfloat16),
        scratch_shapes=[
            pltpu.VMEM((rows_in, NZ * GROUP), jnp.bfloat16),
            pltpu.VMEM((rows_in, WIDE), jnp.float32),
            pltpu.VMEM((NY, rows_in - HALO, WIDE), jnp.float32),
            pltpu.VMEM((rows_in - HALO, NY * WIDE), jnp.bfloat16),
            pltpu.VMEM((NZ, rows_in - HALO, GROUP), jnp.bfloat16),
        ]
        + [
            pltpu.VMEM((SPAN[p["last"]], NC, SPAN[p["outer"]], SPAN[p["inner"]], 3 * DEPTH, WIDE), jnp.bfloat16)
            for p in plans
        ]
        + [
            pltpu.SemaphoreType.DMA((2 * len(p) - 2,)) for p in parts
        ],
        cost_estimate=pl.CostEstimate(
            flops=len(parts) * 6 * rows_in * 2048 * 1024,
            transcendentals=0,
            bytes_accessed=len(parts) * 6 * 2048 * 1024,
        ),
    )(info, x, gain, small, *[a for p in parts for a in p])


def shift(a, axis, by):
    n = SPAN[axis]
    return lax.ppermute(a, axis, [(i, (i + by) % n) for i in range(n)])


def to_each(a, axis):
    return lax.all_to_all(jnp.broadcast_to(a, (SPAN[axis], *a.shape)), axis, 0, 0, tiled=True)


def ring(block, axis):
    n = SPAN[axis]
    held = {0: block}
    up = down = block
    for k in range(1, n // 2):
        up, down = shift(up, axis, 1), shift(down, axis, -1)
        held[n - k], held[k] = up, down
    half = block.shape[0] // 2
    k = n // 2
    farthest = (shift(up[:half], axis, 1), shift(down[half:], axis, -1))
    return held, farthest


def gathered(block, axis):
    held, farthest = ring(block, axis)
    held[SPAN[axis] // 2] = jnp.concatenate(farthest)
    return jnp.stack([held[d] for d in range(SPAN[axis])])


def swapped(a):
    return lax.ppermute(a, "c", [(0, 1), (1, 0)])


def last_parts(block, axis, core):
    n = SPAN[axis]
    parts = [block, swapped(block)]
    moving = jnp.stack(parts)
    axes = ("c", "y") if axis == "y" else (axis, "c")
    at = lambda i, c: c * n + i if axis == "y" else i * NC + c
    route = [(at(i, c), at((i + 1 - 2 * c) % n, c)) for i in range(n) for c in range(NC)]
    for k in range(1, n // 2 + 1):
        if k == n // 2:
            half = block.shape[0] // 2
            moving = lax.dynamic_slice_in_dim(moving, core * half, half, 1)
        moving = lax.ppermute(moving, axes, route)
        parts += [moving, swapped(moving)]
    return parts


def shards(inputs, norm_gain, w_value, w_gate, conv_taps, ln_gain, ln_bias, w_out):
    layers = norm_gain.shape[0]
    rows = inputs.shape[0] // NY
    lead = layers * HALO
    at_z, at_x, core, at_y = (lax.axis_index(a) for a in ("z", "x", "c", "y"))
    at = ((at_z * NX + at_x) * NC + core) * NY + at_y
    firsts = [jnp.maximum((layers - k) * HALO - at * rows, 0) for k in range(layers)]
    info = jnp.stack([at, at_z, at_x, core, *firsts, at_y]).astype(jnp.int32)
    sp = NZ * NX * NC
    before = lax.ppermute(inputs[-lead:], ("z", "x", "c"), [(i, i + 1) for i in range(sp - 1)])
    windows, gain = prepare(info, before, inputs, norm_gain)
    x = lax.all_to_all(windows, "y", 0, 0, tiled=True).reshape(NZ, rows + lead, GROUP)
    own = jnp.concatenate((conv_taps, ln_gain[:, None], ln_bias[:, None]), axis=1)
    small = to_each(own, "y")
    packed = jnp.concatenate((w_value, w_gate, jnp.swapaxes(w_out, 1, 2)), axis=1)
    alone = packed[0]
    xs = jnp.stack([alone, shift(alone, "x", -1), shift(alone, "x", 2), shift(alone, "x", 1)])
    zs = to_each(packed[1:], "z")
    block0 = gathered(xs, "y")
    block0, zs = lax.optimization_barrier((block0, zs))
    zs = lax.dynamic_slice_in_dim(jnp.concatenate((zs, zs)), at_z, NZ)
    block1 = gathered(zs[:, 0], "x")
    block2 = gathered(zs[:, 1], "y")
    parts0 = last_parts(block0, "z", core)
    parts1 = last_parts(block1, "y", core)
    parts2 = last_parts(block2, "x", core)
    x = modules(info, x, gain, small, [parts0], 0)
    x = modules(info, x, gain, small, [parts1, parts2], 1)
    return lax.all_to_all(x, "y", 0, 0, tiled=True).reshape(inputs.shape)


def solution(mesh):
    mesh = Mesh(mesh.devices.reshape(NZ, NX, NC, NY), ("z", "x", "c", "y"))
    sp = ("z", "x", "c")
    in_specs = (
        P(sp, "y"),
        P(),
        P(None, sp, "y"),
        P(None, sp, "y"),
        P(None, None, "y"),
        P(None, "y"),
        P(None, "y"),
        P(None, "y", sp),
    )
    out_specs = P(sp, "y")
    return jax.shard_map(shards, mesh=mesh, in_specs=in_specs, out_specs=out_specs, check_vma=False)
```

```python
import functools

import jax
import jax.numpy as jnp
from jax import lax
from jax.experimental import pallas as pl
from jax.experimental.pallas import tpu as pltpu
from jax.sharding import Mesh, PartitionSpec as P


NZ, NX, NC, NY = 8, 4, 2, 4
HALO = 32
ROWS = 32
TILE = 8
DEPTH, WIDE = 32, 256
GROUP = NX * NC * DEPTH
SPAN = {"z": NZ, "x": NX, "y": NY}

PLANS = (
    dict(last="z", outer="y", inner="x"),
    dict(last="y", outer="x", inner="z"),
    dict(last="x", outer="y", inner="z"),
)


def swap_cores(v, core):
    lane = lax.broadcasted_iota(jnp.int32, v.shape, 1)
    other = jnp.where(
        lane % (2 * DEPTH) < DEPTH,
        pltpu.roll(v, GROUP - DEPTH, 1),
        pltpu.roll(v, DEPTH, 1),
    )
    return jnp.where(core == 1, other, v)


def to_relative(v, at_x, core):
    return swap_cores(pltpu.roll(v, (NX - at_x) * (NC * DEPTH), 1), core)


def to_absolute(v, at_x, core):
    return pltpu.roll(swap_cores(v, core), at_x * (NC * DEPTH), 1)


def prepare_kernel(info_ref, before_ref, x_ref, gain_ref, windows_ref, rel_ref, pad_ref):
    at_z, at_x, core = info_ref[1], info_ref[2], info_ref[3]
    lead = before_ref.shape[0]
    count, halves, window, group = windows_ref.shape
    rows = window - lead
    for half in range(halves):
        cols = slice(half * group, (half + 1) * group)
        pad_ref[:lead] = to_relative(before_ref[:, cols].astype(jnp.float32), at_x, core).astype(jnp.bfloat16)
        for k in range(count):
            turned = to_relative(x_ref[k * rows : (k + 1) * rows, cols].astype(jnp.float32), at_x, core)
            pad_ref[lead + k * rows : lead + (k + 1) * rows] = turned.astype(jnp.bfloat16)
        for k in range(count):
            windows_ref[k, half] = pad_ref[k * rows : k * rows + window]

    def turned_gain(i, carry):
        layer, d = i // NZ, i % NZ
        row = gain_ref[layer, pl.ds((at_z + d) % NZ, 1), :]
        rel_ref[layer, pl.ds(d, 1), :] = to_relative(jnp.broadcast_to(row, (8, group)), at_x, core)[:1]
        return carry

    lax.fori_loop(0, gain_ref.shape[0] * NZ, turned_gain, 0)


def prepare(info, before, x, gain):
    lead, width = before.shape
    rows = x.shape[0] // NY
    return pl.pallas_call(
        prepare_kernel,
        in_specs=[pl.BlockSpec(memory_space=pltpu.SMEM)] + [pl.BlockSpec(memory_space=pltpu.VMEM)] * 3,
        out_specs=[pl.BlockSpec(memory_space=pltpu.VMEM)] * 2,
        out_shape=[
            jax.ShapeDtypeStruct((NY, width // GROUP, rows + lead, GROUP), jnp.bfloat16),
            jax.ShapeDtypeStruct((gain.shape[0], NZ, GROUP), jnp.float32),
        ],
        scratch_shapes=[pltpu.VMEM((lead + x.shape[0], GROUP), jnp.bfloat16)],
        name="prepare",
    )(info, before, x, gain.reshape(-1, NZ, GROUP))


def one_module(layer, reach, info_ref, x_of, gain_ref, small_of, shard, waits, starts, store, hid_ref, glu_ref, fil_ref, norm_ref):
    rows_in = x_of(0).shape[0]
    rows = rows_in - HALO
    channels = NY * WIDE

    def matrix(kind, dy, zs):
        return jnp.concatenate(
            [shard(kind, dy, dz, dx, dc) for dz in zs for dx in range(NX) for dc in range(NC)], axis=0
        )

    def squares(dz, total):
        xf = x_of(dz).astype(jnp.float32)
        return total + jnp.sum(xf * xf, axis=1, keepdims=True)

    total = lax.fori_loop(0, NZ, squares, jnp.zeros((rows_in, 1), jnp.float32))
    scale = lax.rsqrt(total / (NZ * GROUP) + 1e-06)

    def normalised(dz, carry):
        h = x_of(dz).astype(jnp.float32) * scale * gain_ref[layer, pl.ds(dz, 1), :]
        hid_ref[:rows_in, pl.ds(pl.multiple_of(dz * GROUP, GROUP), GROUP)] = h.astype(jnp.bfloat16)
        return carry

    lax.fori_loop(0, NZ, normalised, 0)

    lead = HALO - reach
    row = lax.broadcasted_iota(jnp.int32, (rows_in, 1), 0)
    ahead = row < info_ref[4 + layer]

    def block(dy, carry):
        for k in range(NY):

            @pl.when(dy == k)
            def _():
                for copy in waits[k]:
                    copy.wait()
                for copy in starts[k]:
                    copy.start()

        hidden = hid_ref[:rows_in]
        value = jnp.dot(hidden, matrix(0, dy, range(NZ)), preferred_element_type=jnp.float32)
        gate = jnp.dot(hidden, matrix(1, dy, range(NZ)), preferred_element_type=jnp.float32)
        glu = (value * jax.nn.sigmoid(gate)).astype(jnp.bfloat16).astype(jnp.float32)
        glu_ref[:rows_in] = jnp.where(ahead, 0.0, glu)

        def filtered(i, carry):
            r = pl.multiple_of(i * ROWS, ROWS)
            acc = jnp.zeros((ROWS, WIDE), jnp.float32)
            for s in range(TILE):
                extra = TILE if s else 0
                part = jnp.zeros((ROWS + extra, WIDE), jnp.float32)
                for tap in range(reach + 1):
                    if (tap + lead) % TILE == s:
                        at = pl.multiple_of(r + (tap + lead - s), TILE)
                        part = part + small_of(dy, layer, tap) * glu_ref[pl.ds(at, ROWS + extra), :]
                acc = acc + part[s : s + ROWS]
            fil_ref[dy, pl.ds(r, ROWS), :] = acc
            return carry

        lax.fori_loop(0, rows // ROWS, filtered, 0)
        return carry

    lax.fori_loop(0, NY, block, 0)

    total = jnp.zeros((rows, 1), jnp.float32)
    square = jnp.zeros((rows, 1), jnp.float32)
    for dy in range(NY):
        f = fil_ref[dy, :rows]
        total = total + jnp.sum(f, axis=1, keepdims=True)
        square = square + jnp.sum(f * f, axis=1, keepdims=True)
    mean = total / channels
    scale = lax.rsqrt(square / channels - mean * mean + 1e-06)

    def activated(dy, carry):
        v = (fil_ref[dy, :rows] - mean) * scale * small_of(dy, layer, reach + 1) + small_of(dy, layer, reach + 2)
        cols = pl.ds(pl.multiple_of(dy * WIDE, WIDE), WIDE)
        norm_ref[:rows, cols] = (v * jax.nn.sigmoid(v)).astype(jnp.bfloat16)
        return carry

    lax.fori_loop(0, NY, activated, 0)

    def features(dz, carry):
        weight = jnp.concatenate([matrix(2, dy, (dz,)) for dy in range(NY)], axis=1)
        acc = lax.dot_general(
            norm_ref[:rows], weight, (((1,), (1,)), ((), ())), preferred_element_type=jnp.float32
        )
        store(dz, x_of(dz, HALO).astype(jnp.float32) + acc)
        return carry

    lax.fori_loop(0, NZ, features, 0)


def copies_of(plan, part_refs, held_ref, core, sems):
    n = SPAN[plan["last"]]
    groups = [[(part_refs[0], 0, 0), (part_refs[1], 0, 1)]]
    rest = list(part_refs[2:])
    for k in range(1, n // 2):
        here = jnp.where(core == 0, n - k, k)
        mine, other, rest = rest[:2], rest[2:4], rest[4:]
        groups.append(
            [(mine[0], here, 0), (mine[1], here, 1), (other[0], n - here, 1), (other[1], n - here, 0)]
        )
    groups.append([(rest[0], n // 2, 0), (rest[1], n // 2, 1)])
    pairs = [[(ref, held_ref.at[d, c]) for ref, d, c in group] for group in groups]
    if plan["last"] != "y":
        pairs = [[pair for group in pairs for pair in group]]
    count = iter(range(sems.shape[0]))
    copies = [[pltpu.make_async_copy(*pair, sems.at[next(count)]) for pair in group] for group in pairs]
    return copies + [[]] * (NY - len(copies))


def modules_kernel(first, counts, reach, *refs):
    (info_ref, x_ref, gain_ref, small_ref), refs = refs[:4], refs[4:]
    part_refs = []
    for n in counts:
        part_refs.append(refs[:n])
        refs = refs[n:]
    out_ref, *refs = refs
    work, (mid_ref, *refs) = refs[:4], refs[4:]
    held_refs, sems = refs[: len(counts)], refs[len(counts) :]
    at_z, at_x, core, at_y = info_ref[1], info_ref[2], info_ref[3], info_ref[7]

    copies = [
        copies_of(PLANS[first + k], part_refs[k], held_refs[k], core, sems[k]) for k in range(len(counts))
    ]
    for group in copies[0][:2]:
        for copy in group:
            copy.start()
    starts = [[*groups[2:], [], []] for groups in copies]
    for k, groups in enumerate(copies[1:]):
        starts[k][2] = [copy for group in groups[:2] for copy in group]

    for k in range(len(counts)):
        layer = first + k
        plan, held_ref = PLANS[layer], held_refs[k]
        source = x_ref if k == 0 else mid_ref

        def x_of(dz, skip=0, source=source, layer=layer):
            return source[(at_z + dz) % NZ if layer == 0 else dz, skip:, :]

        def shard(kind, dy, dz, dx, dc, plan=plan, held_ref=held_ref):
            at = dict(x=dx, y=dy, z=dz)
            place = at[plan["last"]], dc, at[plan["outer"]], at[plan["inner"]]
            return held_ref[(*place, slice(kind * DEPTH, (kind + 1) * DEPTH))]

        def store(dz, new, layer=layer, k=k):
            if k < len(counts) - 1:
                mid_ref[dz] = new.astype(jnp.bfloat16)
            elif layer < len(PLANS) - 1:
                out_ref[dz] = new.astype(jnp.bfloat16)
            else:
                z = (at_z + dz) % NZ
                at = pl.multiple_of((z % 2) * GROUP, GROUP)
                out_ref[z // 2, :, pl.ds(at, GROUP)] = to_absolute(new, at_x, core).astype(jnp.bfloat16)

        one_module(
            layer, reach, info_ref, x_of, gain_ref,
            lambda dy, layer, i: small_ref[(at_y + dy) % NY, layer, i : i + 1, :],
            shard, copies[k], starts[k], store, *work,
        )


def modules(info, x, gain, small, parts, first):
    rows_in = x.shape[1]
    rows = rows_in - len(parts) * HALO
    vmem = pl.BlockSpec(memory_space=pltpu.VMEM)
    last = first + len(parts) == len(PLANS)
    plans = PLANS[first : first + len(parts)]
    return pl.pallas_call(
        functools.partial(modules_kernel, first, [len(p) for p in parts], small.shape[2] - 3),
        in_specs=[pl.BlockSpec(memory_space=pltpu.SMEM)]
        + [vmem] * 3
        + [pl.BlockSpec(memory_space=pl.ANY)] * sum(len(p) for p in parts),
        out_specs=vmem,
        out_shape=jax.ShapeDtypeStruct((NZ // 2, rows, 2 * GROUP) if last else (NZ, rows, GROUP), jnp.bfloat16),
        scratch_shapes=[
            pltpu.VMEM((rows_in, NZ * GROUP), jnp.bfloat16),
            pltpu.VMEM((rows_in, WIDE), jnp.float32),
            pltpu.VMEM((NY, rows_in - HALO, WIDE), jnp.float32),
            pltpu.VMEM((rows_in - HALO, NY * WIDE), jnp.bfloat16),
            pltpu.VMEM((NZ, rows_in - HALO, GROUP), jnp.bfloat16),
        ]
        + [
            pltpu.VMEM((SPAN[p["last"]], NC, SPAN[p["outer"]], SPAN[p["inner"]], 3 * DEPTH, WIDE), jnp.bfloat16)
            for p in plans
        ]
        + [
            pltpu.SemaphoreType.DMA((2 * NZ,)) for p in parts
        ],
        cost_estimate=pl.CostEstimate(
            flops=len(parts) * 6 * rows_in * 2048 * 1024,
            transcendentals=0,
            bytes_accessed=len(parts) * 6 * 2048 * 1024,
        ),
    )(info, x, gain, small, *[a for p in parts for a in p])


def shift(a, axis, by):
    n = SPAN[axis]
    return lax.ppermute(a, axis, [(i, (i + by) % n) for i in range(n)])


def to_each(a, axis):
    return lax.all_to_all(jnp.broadcast_to(a, (SPAN[axis], *a.shape)), axis, 0, 0, tiled=True)


def ring(block, axis):
    n = SPAN[axis]
    held = {0: block}
    up = down = block
    for k in range(1, n // 2):
        up, down = shift(up, axis, 1), shift(down, axis, -1)
        held[n - k], held[k] = up, down
    half = block.shape[0] // 2
    k = n // 2
    farthest = (shift(up[:half], axis, 1), shift(down[half:], axis, -1))
    return held, farthest


def gathered(block, axis):
    held, farthest = ring(block, axis)
    held[SPAN[axis] // 2] = jnp.concatenate(farthest)
    return jnp.stack([held[d] for d in range(SPAN[axis])])


def swapped(a):
    return lax.ppermute(a, "c", [(0, 1), (1, 0)])


def last_parts(block, axis):
    n = SPAN[axis]
    axes = ("c", "y") if axis == "y" else (axis, "c")
    at = lambda i, c: c * n + i if axis == "y" else i * NC + c
    route = [(at(i, c), at((i + 1 - 2 * c) % n, c)) for i in range(n) for c in range(NC)]

    def sent(a):
        return lax.ppermute(a, axes, route)

    other = swapped(block)
    parts = [block, other]
    own = block
    for _ in range(1, n // 2):
        own, other = sent(own), sent(other)
        parts += [own, other, swapped(own), swapped(other)]
    own = sent(own)
    return [*parts, own, swapped(own)]


def shards(inputs, norm_gain, w_value, w_gate, conv_taps, ln_gain, ln_bias, w_out):
    layers = norm_gain.shape[0]
    rows = inputs.shape[0] // NY
    lead = layers * HALO
    at_z, at_x, core, at_y = (lax.axis_index(a) for a in ("z", "x", "c", "y"))
    at = ((at_z * NX + at_x) * NC + core) * NY + at_y
    firsts = [jnp.maximum((layers - k) * HALO - at * rows, 0) for k in range(layers)]
    info = jnp.stack([at, at_z, at_x, core, *firsts, at_y]).astype(jnp.int32)
    sp = NZ * NX * NC
    before = lax.ppermute(inputs[-lead:], ("z", "x", "c"), [(i, i + 1) for i in range(sp - 1)])
    windows, gain = prepare(info, before, inputs, norm_gain)
    x = lax.all_to_all(windows, "y", 0, 0, tiled=True).reshape(NZ, rows + lead, GROUP)
    own = jnp.concatenate((conv_taps, ln_gain[:, None], ln_bias[:, None]), axis=1)
    small = to_each(own, "y")
    packed = jnp.concatenate((w_value, w_gate, jnp.swapaxes(w_out, 1, 2)), axis=1)
    xs = to_each(packed[0], "x")
    xs = lax.dynamic_slice_in_dim(jnp.concatenate((xs, xs)), at_x, NX)
    zs = to_each(packed[1:], "z")
    block0 = jnp.stack([xs, shift(xs, "y", -1), shift(xs, "y", 2), shift(xs, "y", 1)])
    block0, zs = lax.optimization_barrier((block0, zs))
    zs = lax.dynamic_slice_in_dim(jnp.concatenate((zs, zs)), at_z, NZ)
    block1 = gathered(zs[:, 0], "x")
    block2 = gathered(zs[:, 1], "y")
    parts0 = last_parts(block0, "z")
    parts1 = last_parts(block1, "y")
    parts2 = last_parts(block2, "x")
    x = modules(info, x, gain, small, [parts0], 0)
    x = modules(info, x, gain, small, [parts1, parts2], 1)
    return lax.all_to_all(x, "y", 0, 0, tiled=True).reshape(inputs.shape)


def solution(mesh):
    mesh = Mesh(mesh.devices.reshape(NZ, NX, NC, NY), ("z", "x", "c", "y"))
    sp = ("z", "x", "c")
    in_specs = (
        P(sp, "y"),
        P(),
        P(None, sp, "y"),
        P(None, sp, "y"),
        P(None, None, "y"),
        P(None, "y"),
        P(None, "y"),
        P(None, "y", sp),
    )
    out_specs = P(sp, "y")
    return jax.shard_map(shards, mesh=mesh, in_specs=in_specs, out_specs=out_specs, check_vma=False)
```

```python
import functools

import jax
import jax.numpy as jnp
from jax import lax
from jax.experimental import pallas as pl
from jax.experimental.pallas import tpu as pltpu
from jax.sharding import Mesh, PartitionSpec as P


NZ, NX, NC, NY = 8, 4, 2, 4
HALO = 32
ROWS = 64
TILE = 8
DEPTH, WIDE = 32, 256
GROUP = NX * NC * DEPTH
SPAN = {"z": NZ, "x": NX, "y": NY}

PLANS = (
    dict(last="z", outer="y", inner="x"),
    dict(last="y", outer="x", inner="z"),
    dict(last="x", outer="y", inner="z"),
)


def swap_cores(v, core):
    lane = lax.broadcasted_iota(jnp.int32, v.shape, 1)
    other = jnp.where(
        lane % (2 * DEPTH) < DEPTH,
        pltpu.roll(v, GROUP - DEPTH, 1),
        pltpu.roll(v, DEPTH, 1),
    )
    return jnp.where(core == 1, other, v)


def to_relative(v, at_x, core):
    return swap_cores(pltpu.roll(v, (NX - at_x) * (NC * DEPTH), 1), core)


def to_absolute(v, at_x, core):
    return pltpu.roll(swap_cores(v, core), at_x * (NC * DEPTH), 1)


def prepare_kernel(info_ref, before_ref, x_ref, gain_ref, windows_ref, rel_ref, pad_ref):
    at_z, at_x, core = info_ref[1], info_ref[2], info_ref[3]
    lead = before_ref.shape[0]
    count, halves, window, group = windows_ref.shape
    rows = window - lead
    for half in range(halves):
        cols = slice(half * group, (half + 1) * group)
        pad_ref[:lead] = to_relative(before_ref[:, cols].astype(jnp.float32), at_x, core).astype(jnp.bfloat16)
        for k in range(count):
            turned = to_relative(x_ref[k * rows : (k + 1) * rows, cols].astype(jnp.float32), at_x, core)
            pad_ref[lead + k * rows : lead + (k + 1) * rows] = turned.astype(jnp.bfloat16)
        for k in range(count):
            windows_ref[k, half] = pad_ref[k * rows : k * rows + window]

    def turned_gain(i, carry):
        layer, d = i // NZ, i % NZ
        row = gain_ref[layer, pl.ds((at_z + d) % NZ, 1), :]
        rel_ref[layer, pl.ds(d, 1), :] = to_relative(jnp.broadcast_to(row, (8, group)), at_x, core)[:1]
        return carry

    lax.fori_loop(0, gain_ref.shape[0] * NZ, turned_gain, 0)


def prepare(info, before, x, gain):
    lead, width = before.shape
    rows = x.shape[0] // NY
    return pl.pallas_call(
        prepare_kernel,
        in_specs=[pl.BlockSpec(memory_space=pltpu.SMEM)] + [pl.BlockSpec(memory_space=pltpu.VMEM)] * 3,
        out_specs=[pl.BlockSpec(memory_space=pltpu.VMEM)] * 2,
        out_shape=[
            jax.ShapeDtypeStruct((NY, width // GROUP, rows + lead, GROUP), jnp.bfloat16),
            jax.ShapeDtypeStruct((gain.shape[0], NZ, GROUP), jnp.float32),
        ],
        scratch_shapes=[pltpu.VMEM((lead + x.shape[0], GROUP), jnp.bfloat16)],
        name="prepare",
    )(info, before, x, gain.reshape(-1, NZ, GROUP))


def one_module(layer, reach, info_ref, x_of, gain_ref, small_of, shard, waits, starts, store, hid_ref, glu_ref, fil_ref, norm_ref):
    rows_in = x_of(0).shape[0]
    rows = rows_in - HALO
    channels = NY * WIDE

    def matrix(kind, dy, zs):
        return jnp.concatenate(
            [shard(kind, dy, dz, dx, dc) for dz in zs for dx in range(NX) for dc in range(NC)], axis=0
        )

    def squares(dz, total):
        xf = x_of(dz).astype(jnp.float32)
        return total + jnp.sum(xf * xf, axis=1, keepdims=True)

    total = lax.fori_loop(0, NZ, squares, jnp.zeros((rows_in, 1), jnp.float32))
    scale = lax.rsqrt(total / (NZ * GROUP) + 1e-06)

    def normalised(dz, carry):
        h = x_of(dz).astype(jnp.float32) * scale * gain_ref[layer, pl.ds(dz, 1), :]
        hid_ref[:rows_in, pl.ds(pl.multiple_of(dz * GROUP, GROUP), GROUP)] = h.astype(jnp.bfloat16)
        return carry

    lax.fori_loop(0, NZ, normalised, 0)

    lead = HALO - reach
    count = max(c for c in range(TILE, ROWS + 1, TILE) if rows % c == 0)
    row = lax.broadcasted_iota(jnp.int32, (rows_in, 1), 0)
    ahead = row < info_ref[4 + layer]

    def block(dy, carry):
        for k in range(NY):

            @pl.when(dy == k)
            def _():
                for copy in waits[k]:
                    copy.wait()
                for copy in starts[k]:
                    copy.start()

        hidden = hid_ref[:rows_in]
        value = jnp.dot(hidden, matrix(0, dy, range(NZ)), preferred_element_type=jnp.float32)
        gate = jnp.dot(hidden, matrix(1, dy, range(NZ)), preferred_element_type=jnp.float32)
        glu = (value * jax.nn.sigmoid(gate)).astype(jnp.bfloat16).astype(jnp.float32)
        glu_ref[:rows_in] = jnp.where(ahead, 0.0, glu)

        def filtered(i, carry):
            r = pl.multiple_of(i * count, count)
            acc = jnp.zeros((count, WIDE), jnp.float32)
            for s in range(TILE):
                extra = TILE if s else 0
                part = jnp.zeros((count + extra, WIDE), jnp.float32)
                for tap in range(reach + 1):
                    if (tap + lead) % TILE == s:
                        at = pl.multiple_of(r + (tap + lead - s), TILE)
                        part = part + small_of(dy, layer, tap) * glu_ref[pl.ds(at, count + extra), :]
                acc = acc + part[s : s + count]
            fil_ref[dy, pl.ds(r, count), :] = acc
            return carry

        lax.fori_loop(0, rows // count, filtered, 0)
        return carry

    lax.fori_loop(0, NY, block, 0)

    total = jnp.zeros((rows, 1), jnp.float32)
    square = jnp.zeros((rows, 1), jnp.float32)
    for dy in range(NY):
        f = fil_ref[dy, :rows]
        total = total + jnp.sum(f, axis=1, keepdims=True)
        square = square + jnp.sum(f * f, axis=1, keepdims=True)
    mean = total / channels
    scale = lax.rsqrt(square / channels - mean * mean + 1e-06)

    def activated(dy, carry):
        v = (fil_ref[dy, :rows] - mean) * scale * small_of(dy, layer, reach + 1) + small_of(dy, layer, reach + 2)
        cols = pl.ds(pl.multiple_of(dy * WIDE, WIDE), WIDE)
        norm_ref[:rows, cols] = (v * jax.nn.sigmoid(v)).astype(jnp.bfloat16)
        return carry

    lax.fori_loop(0, NY, activated, 0)

    def features(dz, carry):
        weight = jnp.concatenate([matrix(2, dy, (dz,)) for dy in range(NY)], axis=1)
        acc = lax.dot_general(
            norm_ref[:rows], weight, (((1,), (1,)), ((), ())), preferred_element_type=jnp.float32
        )
        store(dz, x_of(dz, HALO).astype(jnp.float32) + acc)
        return carry

    lax.fori_loop(0, NZ, features, 0)


def copies_of(plan, part_refs, held_ref, core, sems):
    n = SPAN[plan["last"]]
    groups = [[(part_refs[0], 0, 0), (part_refs[1], 0, 1)]]
    rest = list(part_refs[2:])
    for k in range(1, n // 2):
        here = jnp.where(core == 0, n - k, k)
        mine, other, rest = rest[:2], rest[2:4], rest[4:]
        groups.append(
            [(mine[0], here, 0), (mine[1], here, 1), (other[0], n - here, 1), (other[1], n - here, 0)]
        )
    groups.append([(rest[0], n // 2, 0), (rest[1], n // 2, 1)])
    pairs = [[(ref, held_ref.at[d, c]) for ref, d, c in group] for group in groups]
    if plan["last"] != "y":
        pairs = [[pair for group in pairs for pair in group]]
    count = iter(range(sems.shape[0]))
    copies = [[pltpu.make_async_copy(*pair, sems.at[next(count)]) for pair in group] for group in pairs]
    return copies + [[]] * (NY - len(copies))


def modules_kernel(first, counts, reach, *refs):
    (info_ref, x_ref, gain_ref, small_ref), refs = refs[:4], refs[4:]
    part_refs = []
    for n in counts:
        part_refs.append(refs[:n])
        refs = refs[n:]
    out_ref, *refs = refs
    work, (mid_ref, *refs) = refs[:4], refs[4:]
    held_refs, sems = refs[: len(counts)], refs[len(counts) :]
    at_z, at_x, core, at_y = info_ref[1], info_ref[2], info_ref[3], info_ref[7]

    copies = [
        copies_of(PLANS[first + k], part_refs[k], held_refs[k], core, sems[k]) for k in range(len(counts))
    ]
    for group in copies[0][:2]:
        for copy in group:
            copy.start()
    starts = [[*groups[2:], [], []] for groups in copies]
    for k, groups in enumerate(copies[1:]):
        starts[k][2] = [copy for group in groups[:2] for copy in group]

    for k in range(len(counts)):
        layer = first + k
        plan, held_ref = PLANS[layer], held_refs[k]
        source = x_ref if k == 0 else mid_ref

        def x_of(dz, skip=0, source=source, layer=layer):
            return source[(at_z + dz) % NZ if layer == 0 else dz, skip:, :]

        def shard(kind, dy, dz, dx, dc, plan=plan, held_ref=held_ref):
            at = dict(x=dx, y=dy, z=dz)
            place = at[plan["last"]], dc, at[plan["outer"]], at[plan["inner"]]
            return held_ref[(*place, slice(kind * DEPTH, (kind + 1) * DEPTH))]

        def store(dz, new, layer=layer, k=k):
            if k < len(counts) - 1:
                mid_ref[dz] = new.astype(jnp.bfloat16)
            elif layer < len(PLANS) - 1:
                out_ref[dz] = new.astype(jnp.bfloat16)
            else:
                z = (at_z + dz) % NZ
                at = pl.multiple_of((z % 2) * GROUP, GROUP)
                out_ref[z // 2, :, pl.ds(at, GROUP)] = to_absolute(new, at_x, core).astype(jnp.bfloat16)

        one_module(
            layer, reach, info_ref, x_of, gain_ref,
            lambda dy, layer, i: small_ref[(at_y + dy) % NY, layer, i : i + 1, :],
            shard, copies[k], starts[k], store, *work,
        )


def modules(info, x, gain, small, parts, first):
    rows_in = x.shape[1]
    rows = rows_in - len(parts) * HALO
    vmem = pl.BlockSpec(memory_space=pltpu.VMEM)
    last = first + len(parts) == len(PLANS)
    plans = PLANS[first : first + len(parts)]
    return pl.pallas_call(
        functools.partial(modules_kernel, first, [len(p) for p in parts], small.shape[2] - 3),
        in_specs=[pl.BlockSpec(memory_space=pltpu.SMEM)]
        + [vmem] * 3
        + [pl.BlockSpec(memory_space=pl.ANY)] * sum(len(p) for p in parts),
        out_specs=vmem,
        out_shape=jax.ShapeDtypeStruct((NZ // 2, rows, 2 * GROUP) if last else (NZ, rows, GROUP), jnp.bfloat16),
        scratch_shapes=[
            pltpu.VMEM((rows_in, NZ * GROUP), jnp.bfloat16),
            pltpu.VMEM((rows_in, WIDE), jnp.float32),
            pltpu.VMEM((NY, rows_in - HALO, WIDE), jnp.float32),
            pltpu.VMEM((rows_in - HALO, NY * WIDE), jnp.bfloat16),
            pltpu.VMEM((NZ, rows_in - HALO, GROUP), jnp.bfloat16),
        ]
        + [
            pltpu.VMEM((SPAN[p["last"]], NC, SPAN[p["outer"]], SPAN[p["inner"]], 3 * DEPTH, WIDE), jnp.bfloat16)
            for p in plans
        ]
        + [
            pltpu.SemaphoreType.DMA((2 * NZ,)) for p in parts
        ],
        cost_estimate=pl.CostEstimate(
            flops=len(parts) * 6 * rows_in * 2048 * 1024,
            transcendentals=0,
            bytes_accessed=len(parts) * 6 * 2048 * 1024,
        ),
    )(info, x, gain, small, *[a for p in parts for a in p])


def shift(a, axis, by):
    n = SPAN[axis]
    return lax.ppermute(a, axis, [(i, (i + by) % n) for i in range(n)])


def to_each(a, axis):
    return lax.all_to_all(jnp.broadcast_to(a, (SPAN[axis], *a.shape)), axis, 0, 0, tiled=True)


def ring(block, axis):
    n = SPAN[axis]
    held = {0: block}
    up = down = block
    for k in range(1, n // 2):
        up, down = shift(up, axis, 1), shift(down, axis, -1)
        held[n - k], held[k] = up, down
    half = block.shape[0] // 2
    k = n // 2
    farthest = (shift(up[:half], axis, 1), shift(down[half:], axis, -1))
    return held, farthest


def gathered(block, axis):
    held, farthest = ring(block, axis)
    held[SPAN[axis] // 2] = jnp.concatenate(farthest)
    return jnp.stack([held[d] for d in range(SPAN[axis])])


def swapped(a):
    return lax.ppermute(a, "c", [(0, 1), (1, 0)])


def last_parts(block, axis):
    n = SPAN[axis]
    axes = ("c", "y") if axis == "y" else (axis, "c")
    at = lambda i, c: c * n + i if axis == "y" else i * NC + c
    route = [(at(i, c), at((i + 1 - 2 * c) % n, c)) for i in range(n) for c in range(NC)]

    def sent(a):
        return lax.ppermute(a, axes, route)

    other = swapped(block)
    parts = [block, other]
    own = block
    for _ in range(1, n // 2):
        own, other = sent(own), sent(other)
        parts += [own, other, swapped(own), swapped(other)]
    own = sent(own)
    return [*parts, own, swapped(own)]


def shards(inputs, norm_gain, w_value, w_gate, conv_taps, ln_gain, ln_bias, w_out):
    layers = norm_gain.shape[0]
    rows = inputs.shape[0] // NY
    lead = layers * HALO
    at_z, at_x, core, at_y = (lax.axis_index(a) for a in ("z", "x", "c", "y"))
    at = ((at_z * NX + at_x) * NC + core) * NY + at_y
    firsts = [jnp.maximum((layers - k) * HALO - at * rows, 0) for k in range(layers)]
    info = jnp.stack([at, at_z, at_x, core, *firsts, at_y]).astype(jnp.int32)
    sp = NZ * NX * NC
    before = lax.ppermute(inputs[-lead:], ("z", "x", "c"), [(i, i + 1) for i in range(sp - 1)])
    windows, gain = prepare(info, before, inputs, norm_gain)
    x = lax.all_to_all(windows, "y", 0, 0, tiled=True).reshape(NZ, rows + lead, GROUP)
    own = jnp.concatenate((conv_taps, ln_gain[:, None], ln_bias[:, None]), axis=1)
    small = to_each(own, "y")
    packed = jnp.concatenate((w_value, w_gate, jnp.swapaxes(w_out, 1, 2)), axis=1)
    xs = to_each(packed[0], "x")
    xs = lax.dynamic_slice_in_dim(jnp.concatenate((xs, xs)), at_x, NX)
    zs = to_each(packed[1:], "z")
    block0 = jnp.stack([xs, shift(xs, "y", -1), shift(xs, "y", 2), shift(xs, "y", 1)])
    block0, zs = lax.optimization_barrier((block0, zs))
    zs = lax.dynamic_slice_in_dim(jnp.concatenate((zs, zs)), at_z, NZ)
    block1 = gathered(zs[:, 0], "x")
    block2 = gathered(zs[:, 1], "y")
    parts0 = last_parts(block0, "z")
    parts1 = last_parts(block1, "y")
    parts2 = last_parts(block2, "x")
    x = modules(info, x, gain, small, [parts0], 0)
    x = modules(info, x, gain, small, [parts1, parts2], 1)
    return lax.all_to_all(x, "y", 0, 0, tiled=True).reshape(inputs.shape)


def solution(mesh):
    mesh = Mesh(mesh.devices.reshape(NZ, NX, NC, NY), ("z", "x", "c", "y"))
    sp = ("z", "x", "c")
    in_specs = (
        P(sp, "y"),
        P(),
        P(None, sp, "y"),
        P(None, sp, "y"),
        P(None, None, "y"),
        P(None, "y"),
        P(None, "y"),
        P(None, "y", sp),
    )
    out_specs = P(sp, "y")
    return jax.shard_map(shards, mesh=mesh, in_specs=in_specs, out_specs=out_specs, check_vma=False)
```
